32 devices in a mesh: sp: 4 (over z), dp: 8 (over y, x, core).
Axes of the slice: x: 2, y: 2, z: 4, core: 2. Of those that a mesh axis runs over, the one named last changes fastest.
Arguments:
- query_latent: bfloat16 [8, 512, 768], P('dp', 'sp'), may hold values from -6 to 6
- keyvalue_latent: bfloat16 [8, 512, 512], P('dp', 'sp'), may hold values from -6 to 6
- rope_key: bfloat16 [8, 512, 32], P('dp', 'sp'), may hold values from -150 to 150
- query_gain: float32 [768], replicated, may hold values from 0.1 to 1.9
- keyvalue_gain: float32 [512], replicated, may hold values from 0.1 to 1.9
- narrow_query: bfloat16 [768, 384], P('dp'), may hold values from -0.21875 to 0.21875
- broad_query: bfloat16 [768, 640], P('dp'), may hold values from -0.21875 to 0.21875
- narrow_key: bfloat16 [512, 256], P('dp'), may hold values from -0.25 to 0.25
- narrow_value: bfloat16 [512, 256], P('dp'), may hold values from -0.25 to 0.25
- broad_key: bfloat16 [512, 512], P('dp'), may hold values from -0.25 to 0.25
- broad_value: bfloat16 [512, 256], P('dp'), may hold values from -0.25 to 0.25
Outputs:
- narrow_mixed: bfloat16 [8, 512, 256], P('dp', 'sp')
- broad_mixed: bfloat16 [8, 512, 256], P('dp', 'sp')
The draws below stay inside these ranges and needn't reach their ends.
All inputs are finite; a program needn't handle non-finite values.
Results may differ from the reference program's by a relative error of at most 0.014.
The reference program's roundings to bfloat16 on the way count: a program that leaves them out, or rounds other values in their place, can miss the bound.
Values may be sent and summed in bfloat16 or wider, within the bound.
A program may use at most 64 MiB of HBM per device.

```python
import jax
import jax.numpy as jnp
from jax import lax

QUERY_RANK = 768
PAIR_RANK = 512
PLAIN_NARROW = 64
PLAIN_BROAD = 128
ROTARY = 32
VALUE_SIZE = 64
HEADS = 4
LENGTH = 512
SEQS = 8


def draw_rope_key(key, part):
    base_key = jax.random.fold_in(key, 11)
    values = jnp.clip(jax.random.normal(base_key, (SEQS, LENGTH, ROTARY), jnp.float32), -6.0, 6.0)
    return values.astype(jnp.bfloat16)


def level_of(key, shape, split, smallest, high):
    loudness = 1.0
    for position, shards_of in split:
        draws = jax.random.uniform(jax.random.fold_in(jax.random.fold_in(key, 6), position), (shards_of,), jnp.float32, smallest / len(split), high / len(split))
        loudness = loudness * jnp.repeat(jnp.exp(draws), shape[position] // shards_of).reshape((-1,) + (1,) * (len(shape) - 1 - position))
    return loudness


def normal_values(rng, extent, spread, limit, shards=(), held_as=jnp.bfloat16):
    array = spread * jax.random.normal(rng, extent, jnp.float32)
    if shards:
        array = array * level_of(rng, extent, shards, -0.22, 0.18)
    return jnp.clip(array, -limit, limit).astype(held_as)


def setup_inputs(seed: int = 0) -> dict:
    arg_keys = jax.random.split(jax.random.key(seed), 12)
    return {
        "query_latent": normal_values(arg_keys[0], (SEQS, LENGTH, QUERY_RANK), 1.0, 6.0, ((0, 8), (1, 4))),
        "keyvalue_latent": normal_values(arg_keys[1], (SEQS, LENGTH, PAIR_RANK), 1.0, 6.0, ((0, 8), (1, 4))),
        "rope_key": draw_rope_key(jax.random.fold_in(arg_keys[11], 71), 0),
        "query_gain": jnp.clip(1.0 + 0.18 * jax.random.normal(arg_keys[3], (QUERY_RANK,), jnp.float32), 0.1, 1.9),
        "keyvalue_gain": jnp.clip(1.0 + 0.18 * jax.random.normal(arg_keys[4], (PAIR_RANK,), jnp.float32), 0.1, 1.9),
        "narrow_query": normal_values(arg_keys[5], (QUERY_RANK, HEADS * (PLAIN_NARROW + ROTARY)), QUERY_RANK ** -0.5, 0.21875, ((0, 8),)),
        "broad_query": normal_values(arg_keys[6], (QUERY_RANK, HEADS * (PLAIN_BROAD + ROTARY)), QUERY_RANK ** -0.5, 0.21875, ((0, 8),)),
        "narrow_key": normal_values(arg_keys[7], (PAIR_RANK, HEADS * PLAIN_NARROW), PAIR_RANK ** -0.5, 0.25, ((0, 8),)),
        "narrow_value": normal_values(arg_keys[8], (PAIR_RANK, HEADS * VALUE_SIZE), PAIR_RANK ** -0.5, 0.25, ((0, 8),)),
        "broad_key": normal_values(arg_keys[9], (PAIR_RANK, HEADS * PLAIN_BROAD), PAIR_RANK ** -0.5, 0.25, ((0, 8),)),
        "broad_value": normal_values(arg_keys[10], (PAIR_RANK, HEADS * VALUE_SIZE), PAIR_RANK ** -0.5, 0.25, ((0, 8),)),
    }


EPSILON = 1e-06
ROTARY_BASE = 10000.0

def normalize(latent, gain_row):
    values = latent.astype(jnp.float32)
    scaled = values * lax.rsqrt(lax.optimization_barrier(jnp.mean(values * values, axis=-1, keepdims=True)) + EPSILON)
    return (scaled * gain_row.astype(jnp.float32)).astype(jnp.bfloat16)

def rotate(values, positions):
    halfway = ROTARY // 2
    frequency = ROTARY_BASE ** (-jnp.arange(halfway, dtype=jnp.float32) / halfway)
    angles = positions[:, None] * frequency[None, :]
    cosine = jnp.cos(angles)[:, None, :]
    sine_part = jnp.sin(angles)[:, None, :]
    width = values.shape[-1]
    plain_part = values[..., :width - ROTARY]
    first_half = values[..., width - ROTARY:width - halfway]
    second_half = values[..., width - halfway:]
    return jnp.concatenate([plain_part, first_half * cosine - second_half * sine_part, first_half * sine_part + second_half * cosine], axis=-1)

def attend_group(queries, keys_plain, values, rope_keys, factor):

    def one_head(members):
        query_head, key_head, value_head = members
        key_whole = jnp.concatenate([key_head, rope_keys], axis=1)
        scores = jnp.dot(query_head, key_whole.T, preferred_element_type=jnp.float32) * factor
        shifted = jnp.exp(scores - lax.optimization_barrier(jnp.max(scores, axis=-1, keepdims=True)))
        totals = lax.optimization_barrier(jnp.sum(shifted, axis=-1, keepdims=True))
        mixed = jnp.dot(shifted.astype(jnp.bfloat16), value_head, preferred_element_type=jnp.float32)
        return (mixed / totals).astype(jnp.bfloat16)
    stacked = lax.map(one_head, (jnp.swapaxes(queries, 0, 1), jnp.swapaxes(keys_plain, 0, 1), jnp.swapaxes(values, 0, 1)))
    return jnp.swapaxes(stacked, 0, 1)

def group_norm(attended):
    flattened = attended.reshape(attended.shape[0], -1).astype(jnp.float32)
    scaled = flattened * lax.rsqrt(lax.optimization_barrier(jnp.mean(flattened * flattened, axis=-1, keepdims=True)) + EPSILON)
    return scaled.astype(jnp.bfloat16)

def reference(query_latent, keyvalue_latent, rope_key, query_gain, keyvalue_gain, narrow_query, broad_query, narrow_key, narrow_value, broad_key, broad_value):

    def one_sequence(members):
        query_rows, pair_rows, rope_rows = members
        length = query_rows.shape[0]
        positions = jnp.arange(length).astype(jnp.float32)
        query_normed = normalize(query_rows, query_gain)
        pair_normed = normalize(pair_rows, keyvalue_gain)
        rope_keys = rotate(rope_rows.astype(jnp.float32)[:, None, :], positions)[:, 0, :].astype(jnp.bfloat16)
        width_narrow = PLAIN_NARROW + ROTARY
        width_broad = PLAIN_BROAD + ROTARY
        query_first = rotate(jnp.dot(query_normed, narrow_query, preferred_element_type=jnp.float32).reshape(length, HEADS, width_narrow), positions).astype(jnp.bfloat16)
        query_second = rotate(jnp.dot(query_normed, broad_query, preferred_element_type=jnp.float32).reshape(length, HEADS, width_broad), positions).astype(jnp.bfloat16)
        key_first = jnp.dot(pair_normed, narrow_key, preferred_element_type=jnp.float32).astype(jnp.bfloat16).reshape(length, HEADS, PLAIN_NARROW)
        value_first = jnp.dot(pair_normed, narrow_value, preferred_element_type=jnp.float32).astype(jnp.bfloat16).reshape(length, HEADS, VALUE_SIZE)
        key_second = jnp.dot(pair_normed, broad_key, preferred_element_type=jnp.float32).astype(jnp.bfloat16).reshape(length, HEADS, PLAIN_BROAD)
        value_second = jnp.dot(pair_normed, broad_value, preferred_element_type=jnp.float32).astype(jnp.bfloat16).reshape(length, HEADS, VALUE_SIZE)
        mixed_first = attend_group(query_first, key_first, value_first, rope_keys, width_narrow ** (-0.5))
        mixed_second = attend_group(query_second, key_second, value_second, rope_keys, width_broad ** (-0.5))
        return (group_norm(mixed_first), group_norm(mixed_second))
    narrow_mixed, broad_mixed = lax.map(one_sequence, (query_latent, keyvalue_latent, rope_key))
    return (narrow_mixed, broad_mixed)
```

```python
import functools
import math

import jax
import jax.numpy as jnp
import numpy as np
from jax import lax
from jax.experimental import pallas as pl
from jax.experimental.pallas import tpu as pltpu
from jax.sharding import PartitionSpec as P

PLAIN_NARROW = 64
PLAIN_BROAD = 128
ROTARY = 32
VALUE_SIZE = 64


EPSILON = 1e-06
ROTARY_BASE = 10000.0


def normalize(latent, gain_row):
    values = latent.astype(jnp.float32)
    scaled = values * lax.rsqrt(jnp.mean(values * values, axis=-1, keepdims=True) + EPSILON)
    return (scaled * gain_row).astype(jnp.bfloat16)


def rotate(values, positions):
    halfway = ROTARY // 2
    frequency = ROTARY_BASE ** (-jnp.arange(halfway, dtype=jnp.float32) / halfway)
    angles = positions[:, None] * frequency[None, :]
    cosine = jnp.cos(angles)[:, None, :]
    sine_part = jnp.sin(angles)[:, None, :]
    width = values.shape[-1]
    plain_part = values[..., : width - ROTARY]
    first_half = values[..., width - ROTARY : width - halfway]
    second_half = values[..., width - halfway :]
    return jnp.concatenate(
        [
            plain_part,
            first_half * cosine - second_half * sine_part,
            first_half * sine_part + second_half * cosine,
        ],
        axis=-1,
    )


def make_fold(latent, pieces):
    return tuple(
        (jnp.dot(latent, weight_rows, preferred_element_type=jnp.float32) for weight_rows in pieces)
    )


def arrange(sums, width, positions, groups, with_rotary):
    row_count = positions.shape[0]
    shaped = sums.reshape(row_count, -1, width)
    if with_rotary:
        shaped = rotate(shaped, positions)
    shaped = shaped.astype(jnp.bfloat16)
    return shaped.reshape(row_count, groups, shaped.shape[1] // groups, width)


def attend_group(queries, keys_plain, values, rope_keys, factor):
    length = queries.shape[0]
    block_rows = 512
    key_whole = jnp.concatenate([keys_plain[:, 0, :], rope_keys], axis=1)
    value_head = values[:, 0, :]

    def one_block(query_block):
        scores = (
            jnp.einsum("qd,kd->qk", query_block, key_whole, preferred_element_type=jnp.float32)
            * factor
        )
        shifted = jnp.exp(scores - jnp.max(scores, axis=-1, keepdims=True))
        totals = jnp.sum(shifted, axis=-1, keepdims=True)
        mixed = jnp.dot(
            shifted.astype(jnp.bfloat16), value_head, preferred_element_type=jnp.float32
        )
        return (mixed / totals).astype(jnp.bfloat16)

    blocks = lax.map(one_block, queries[:, 0, :].reshape(length // block_rows, block_rows, -1))
    results = [blocks.reshape(length, -1)]
    return jnp.stack(results, axis=1)


def attend_both(members, rope_keys):
    query_first, key_first, value_first, query_second, key_second, value_second = members
    mixed_first = attend_group(
        query_first[:, 0],
        key_first[:, 0],
        value_first[:, 0],
        rope_keys,
        (PLAIN_NARROW + ROTARY) ** (-0.5),
    )
    mixed_second = attend_group(
        query_second[:, 0],
        key_second[:, 0],
        value_second[:, 0],
        rope_keys,
        (PLAIN_BROAD + ROTARY) ** (-0.5),
    )
    return (mixed_first[:, None], mixed_second[:, None])


def finish(mixed):
    flattened = mixed.reshape(mixed.shape[0], -1).astype(jnp.float32)
    scaled = flattened * lax.rsqrt(
        jnp.mean(flattened * flattened, axis=-1, keepdims=True) + EPSILON
    )
    return scaled.astype(jnp.bfloat16)[None]


def on_device(
    query_latent,
    keyvalue_latent,
    rope_key,
    query_gain,
    keyvalue_gain,
    narrow_query,
    broad_query,
    narrow_key,
    narrow_value,
    broad_key,
    broad_value,
):
    tokens = query_latent.shape[1]
    spread = lax.axis_size("sp")
    device_index = lax.axis_index("sp")
    width_narrow = PLAIN_NARROW + ROTARY
    width_broad = PLAIN_BROAD + ROTARY
    query_normed = normalize(query_latent[0], query_gain)
    pair_normed = normalize(keyvalue_latent[0], keyvalue_gain)
    own_positions = (device_index * tokens + jnp.arange(tokens, dtype=jnp.int32)).astype(
        jnp.float32
    )
    rope_own = rotate(rope_key[0].astype(jnp.float32)[:, None, :], own_positions)[:, 0, :].astype(
        jnp.bfloat16
    )
    query_all, pair_all, rope_all = (
        lax.all_gather(query_normed, "sp", axis=0, tiled=True),
        lax.all_gather(pair_normed, "sp", axis=0, tiled=True),
        lax.all_gather(rope_own, "sp", axis=0, tiled=True),
    )
    length = tokens * spread
    all_positions = jnp.arange(length, dtype=jnp.int32).astype(jnp.float32)

    def own_columns(weight, width):
        count = weight.shape[1] // (width * spread)
        return lax.dynamic_slice_in_dim(weight, device_index * count * width, count * width, 1)

    own_narrow_query = own_columns(narrow_query, width_narrow)
    own_broad_query = own_columns(broad_query, width_broad)
    own_narrow_key = own_columns(narrow_key, PLAIN_NARROW)
    own_narrow_value = own_columns(narrow_value, VALUE_SIZE)
    own_broad_key = own_columns(broad_key, PLAIN_BROAD)
    own_broad_value = own_columns(broad_value, VALUE_SIZE)
    query_sums = make_fold(
        query_all,
        (
            lax.all_gather(own_narrow_query, "dp", axis=0, tiled=True),
            lax.all_gather(own_broad_query, "dp", axis=0, tiled=True),
        ),
    )
    pair_sums = make_fold(
        pair_all,
        (
            lax.all_gather(own_narrow_key, "dp", axis=0, tiled=True),
            lax.all_gather(own_narrow_value, "dp", axis=0, tiled=True),
            lax.all_gather(own_broad_key, "dp", axis=0, tiled=True),
            lax.all_gather(own_broad_value, "dp", axis=0, tiled=True),
        ),
    )
    members = (
        arrange(query_sums[0], width_narrow, all_positions, 1, True),
        arrange(pair_sums[0], PLAIN_NARROW, all_positions, 1, False),
        arrange(pair_sums[1], VALUE_SIZE, all_positions, 1, False),
        arrange(query_sums[1], width_broad, all_positions, 1, True),
        arrange(pair_sums[2], PLAIN_BROAD, all_positions, 1, False),
        arrange(pair_sums[3], VALUE_SIZE, all_positions, 1, False),
    )
    mixed_first, mixed_second = attend_both(members, rope_all)
    back_first, back_second = (
        lax.all_to_all(mixed_first, "sp", split_axis=0, concat_axis=1, tiled=True),
        lax.all_to_all(mixed_second, "sp", split_axis=0, concat_axis=1, tiled=True),
    )
    return (finish(back_first), finish(back_second))


MESH = pl.DeviceIdType.MESH
ROW_TILE = 16
LANES = 128
NK, NV, BK, BV, NQ, BQ = range(6)
KINDS = 9


def rotary_tables(length):
    halfway = ROTARY // 2
    frequency = (
        np.float32(ROTARY_BASE) ** (-np.arange(halfway, dtype=np.float32) / np.float32(halfway))
    ).astype(np.float32)
    angles = np.arange(length, dtype=np.float32)[:, None] * frequency[None, :]
    cosine = np.cos(angles.astype(np.float64)).astype(np.float32)
    sine = np.sin(angles.astype(np.float64)).astype(np.float32)
    return cosine, sine


def key_table(length):
    cosine, sine = rotary_tables(length)
    return np.concatenate([cosine, cosine, -sine, sine], 1)


def wide_tables(table, plain, heads):
    rows, halfway = table.shape[0], ROTARY // 2
    ones = jnp.ones((rows, plain), jnp.float32)
    zeros = jnp.zeros((rows, plain), jnp.float32)
    zero = jnp.zeros((rows, halfway), jnp.float32)
    keep = [ones, table[:, :ROTARY]]
    ahead = [zeros, table[:, ROTARY : ROTARY + halfway], zero]
    behind = [zeros, zero, table[:, ROTARY + halfway :]]
    return [jnp.concatenate(parts * heads, axis=1) for parts in (keep, ahead, behind)]


def fused(
    spread,
    heads,
    query_hbm,
    pair_hbm,
    rope_hbm,
    qgain_hbm,
    pgain_hbm,
    w0,
    w1,
    w2,
    w3,
    w4,
    w5,
    ktab_hbm,
    narrow_out,
    broad_out,
    g0,
    g1,
    g2,
    g3,
    g4,
    g5,
    query_buf,
    pair_buf,
    rope_buf,
    qgain,
    pgain,
    ntab,
    btab,
    ktab,
    pair_normed,
    rope_keys,
    send_sem,
    recv_sem,
    zsend_sem,
    zrecv_sem,
    local_sem,
    wlocal_sem,
):
    weights = (w0, w1, w2, w3, w4, w5)
    gathered = (g0, g1, g2, g3, g4, g5)
    tokens = query_hbm.shape[1]
    z = lax.axis_index("sp")
    me = lax.axis_index("dp")
    core = me % 2
    flip_p = 1 - 2 * core
    flip_x = 2 * (1 - 2 * ((me // 2) % 2))
    flip_y = 4 * (1 - 2 * (me // 4))
    peer_p, peer_x, peer_y = me + flip_p, me + flip_x, me + flip_y
    diagonal = me + flip_x + flip_y

    columns_all = [w.shape[1] for w in weights]
    pieces = [(a, 0, columns_all[a]) for a in (NK, NV, BK, BV, NQ)]
    split = -(-(columns_all[BQ] // 2) // LANES) * LANES
    pieces += [(BQ, 0, split), (BQ, split, columns_all[BQ] - split)]

    local = [
        pltpu.make_async_copy(pair_hbm.at[0], pair_buf.at[z], local_sem.at[0]),
        pltpu.make_async_copy(rope_hbm.at[0], rope_buf.at[z], local_sem.at[1]),
        pltpu.make_async_copy(query_hbm.at[0], query_buf, local_sem.at[2]),
        pltpu.make_async_copy(qgain_hbm, qgain, local_sem.at[3]),
        pltpu.make_async_copy(pgain_hbm, pgain, local_sem.at[4]),
        pltpu.make_async_copy(ktab_hbm, ktab, local_sem.at[5]),
    ]

    def rows_of(array, owner, half=None):
        rows = weights[array].shape[0]
        if half is None:
            return pl.ds(pl.multiple_of(owner * rows, rows), rows)
        part = rows // 2
        return pl.ds(pl.multiple_of(owner * rows + half * part, part), part)

    own_weights = [
        pltpu.make_async_copy(
            weights[a], gathered[a].at[rows_of(a, me)], wlocal_sem.at[a]
        )
        for a in range(len(weights))
    ]
    for copy in local + own_weights:
        copy.start()

    barrier = pltpu.get_barrier_semaphore()
    for peer in (peer_p, peer_x, peer_y):
        pl.semaphore_signal(barrier, inc=1, device_id=(z, peer), device_id_type=MESH)

    @pl.when(z > 0)
    def _():
        pl.semaphore_signal(barrier, inc=1, device_id=(z - 1, me), device_id_type=MESH)

    @pl.when(z < spread - 1)
    def _():
        pl.semaphore_signal(barrier, inc=1, device_id=(z + 1, me), device_id_type=MESH)

    line = (z + spread - 1) // spread + (2 * spread - 2 - z) // spread
    pl.semaphore_wait(barrier, 3 + line)

    chunks = 2
    chunk_rows = tokens // chunks

    def along(item, owner, step, own):
        if item < chunks:
            rows = pl.ds(item * chunk_rows, chunk_rows)
            target = pair_buf.at[owner, rows]
            source = pair_hbm.at[0, rows] if own else target
        else:
            target = rope_buf.at[owner]
            source = rope_hbm.at[0] if own else target
        return pltpu.make_async_remote_copy(
            src_ref=source,
            dst_ref=target,
            send_sem=zsend_sem.at[0 if step < 0 else 1, owner, item],
            recv_sem=zrecv_sem.at[owner, item],
            device_id=(z + step, me),
            device_id_type=MESH,
        )

    def send_along(owner, own, step, item):
        @pl.when((z > 0) if step < 0 else (z < spread - 1))
        def _():
            along(item, owner, step, own).start()

    items = range(chunks + 1)
    for item in items:
        for step in (-1, 1):
            send_along(z, True, step, item)

    def relay_along(distance, item):
        for side in (1, -1):
            owner = z + side * distance

            @pl.when((owner >= 0) & (owner < spread))
            def _():
                along(item, owner, -side, False).wait_recv()
                send_along(owner, False, -side, item)

    def across(index, kind):
        a, start, width = pieces[index]
        cols = pl.ds(start, width)
        target_of = {
            0: (me, None, peer_p),
            1: (me, None, peer_x),
            2: (me, None, peer_y),
            3: (peer_x, None, peer_p),
            4: (peer_y, None, peer_p),
            5: (peer_x, 0, peer_y),
            6: (peer_y, 1, peer_x),
            7: (diagonal, 0, peer_p),
            8: (diagonal, 1, peer_p),
        }
        owner, half, device = target_of[kind]
        target = gathered[a].at[rows_of(a, owner, half), cols]
        source = weights[a].at[:, cols] if kind < 3 else target
        return pltpu.make_async_remote_copy(
            src_ref=source,
            dst_ref=target,
            send_sem=send_sem.at[index, kind],
            recv_sem=recv_sem.at[index, kind],
            device_id=(z, device),
            device_id_type=MESH,
        )

    def arrived(index, kind):
        a, start, width = pieces[index]
        owner, half = {
            0: (peer_p, None),
            1: (peer_x, None),
            2: (peer_y, None),
            3: (peer_x + flip_p, None),
            4: (peer_y + flip_p, None),
            5: (diagonal, 0),
            6: (diagonal, 1),
            7: (diagonal + flip_p, 0),
            8: (diagonal + flip_p, 1),
        }[kind]
        target = gathered[a].at[rows_of(a, owner, half), pl.ds(start, width)]
        pltpu.make_async_remote_copy(
            src_ref=target,
            dst_ref=target,
            send_sem=send_sem.at[index, kind],
            recv_sem=recv_sem.at[index, kind],
            device_id=(z, peer_p),
            device_id_type=MESH,
        ).wait_recv()

    def send_own(index):
        for kind in (1, 2, 0):
            across(index, kind).start()

    def relay(index):
        arrived(index, 1)
        across(index, 5).start()
        across(index, 3).start()
        arrived(index, 2)
        across(index, 6).start()
        across(index, 4).start()

    def hand_over(index):
        for half in (0, 1):
            arrived(index, 5 + half)
            across(index, 7 + half).start()

    def complete(index):
        for kind in (0, 3, 4, 7, 8):
            arrived(index, kind)

    for index in range(4):
        send_own(index)

    def normed(values, gain):
        values = values.astype(jnp.float32)
        scaled = values * lax.rsqrt(jnp.mean(values * values, axis=-1, keepdims=True) + EPSILON)
        return (scaled * gain).astype(jnp.bfloat16)

    for copy in local:
        copy.wait()
    for copy in own_weights:
        copy.wait()
    query_normed = normed(query_buf[...], qgain[...])
    own_table = ktab[pl.ds(pl.multiple_of(z * tokens, tokens), tokens)]
    for table, plain in ((ntab, PLAIN_NARROW), (btab, PLAIN_BROAD)):
        for index, values in enumerate(wide_tables(own_table, plain, heads)):
            table[index] = values

    relay(0)
    send_own(4)
    for item in items:
        relay_along(1, item)
    relay(1)
    relay(2)
    relay(3)
    hand_over(0)
    send_own(5)
    send_own(6)
    hand_over(1)
    hand_over(2)
    for distance in range(2, spread):
        for item in items:
            relay_along(distance, item)
    hand_over(3)
    relay(4)
    relay(5)
    relay(6)
    for index in range(4):
        complete(index)

    for block in range(spread):
        rows = pl.ds(block * tokens, tokens)
        pair_normed[rows] = normed(pair_buf[block], pgain[...])
        plain = rope_buf[block].astype(jnp.float32)
        halfway = ROTARY // 2
        swapped = jnp.concatenate([plain[:, halfway:], plain[:, :halfway]], axis=1)
        rope_keys[rows] = (
            plain * ktab[rows, :ROTARY] + swapped * ktab[rows, ROTARY:]
        ).astype(jnp.bfloat16)

    def product(left, right):
        return jnp.dot(left, right, preferred_element_type=jnp.float32)

    narrow_keys = product(pair_normed[...], g0[...]).astype(jnp.bfloat16)
    narrow_values = product(pair_normed[...], g1[...]).astype(jnp.bfloat16)
    hand_over(4)
    broad_keys = product(pair_normed[...], g2[...]).astype(jnp.bfloat16)
    broad_values = product(pair_normed[...], g3[...]).astype(jnp.bfloat16)
    hand_over(5)
    hand_over(6)

    def attend(query_weights, table, keys, values, plain, out):
        width = plain + ROTARY
        sums = product(query_normed, query_weights[...])
        total = sums.shape[1]
        halfway = ROTARY // 2
        queries = (
            sums * table[0]
            + pltpu.roll(sums, total - halfway, 1) * table[1]
            + pltpu.roll(sums, halfway, 1) * table[2]
        ).astype(jnp.bfloat16)
        factor = width ** (-0.5) * math.log2(math.e)
        attended = []
        for head in range(heads):
            query = queries[:, head * width : (head + 1) * width]
            key = jnp.concatenate(
                [keys[:, head * plain : (head + 1) * plain], rope_keys[...]], axis=1
            )
            scores = lax.dot_general(
                query, key, (((1,), (1,)), ((), ())), preferred_element_type=jnp.float32
            )
            shifted = jnp.exp2((scores - jnp.max(scores, axis=-1, keepdims=True)) * factor)
            totals = jnp.sum(shifted, axis=-1, keepdims=True)
            mixed = product(
                shifted.astype(jnp.bfloat16), values[:, head * VALUE_SIZE : (head + 1) * VALUE_SIZE]
            )
            attended.append((mixed / totals).astype(jnp.bfloat16).astype(jnp.float32))
        flat = jnp.concatenate(attended, axis=1)
        scaled = flat * lax.rsqrt(jnp.mean(flat * flat, axis=-1, keepdims=True) + EPSILON)
        out[0] = scaled.astype(jnp.bfloat16)

    complete(4)
    attend(g4, ntab, narrow_keys, narrow_values, PLAIN_NARROW, narrow_out)
    complete(5)
    complete(6)
    attend(g5, btab, broad_keys, broad_values, PLAIN_BROAD, broad_out)

    for index in range(len(pieces)):
        for kind in range(KINDS):
            across(index, kind).wait_send()
    for item in items:
        for step in (-1, 1):
            for distance in range(spread):
                owner = z - step * distance

                @pl.when(
                    (owner >= 0)
                    & (owner < spread)
                    & ((z > 0) if step < 0 else (z < spread - 1))
                )
                def _():
                    along(item, owner, step, False).wait_send()


def fused_call(
    spread,
    query_latent,
    keyvalue_latent,
    rope_key,
    query_gain,
    keyvalue_gain,
    narrow_query,
    broad_query,
    narrow_key,
    narrow_value,
    broad_key,
    broad_value,
):
    tokens, query_rank = query_latent.shape[1:]
    pair_rank = keyvalue_latent.shape[2]
    length = tokens * spread
    heads = narrow_value.shape[1] // VALUE_SIZE
    weights = (narrow_key, narrow_value, broad_key, broad_value, narrow_query, broad_query)
    peers = lax.axis_size("dp")
    ktab = key_table(length)
    operands = (
        query_latent,
        keyvalue_latent,
        rope_key,
        query_gain[None],
        keyvalue_gain[None],
        *weights,
        jnp.asarray(ktab),
    )
    out = jax.ShapeDtypeStruct((1, tokens, heads * VALUE_SIZE), jnp.bfloat16)
    bf16, f32 = jnp.bfloat16, jnp.float32
    return pl.pallas_call(
        functools.partial(fused, spread, heads),
        out_shape=(out, out),
        in_specs=[pl.BlockSpec(memory_space=pl.ANY)] * len(operands),
        out_specs=[pl.BlockSpec(memory_space=pltpu.VMEM)] * 2,
        scratch_shapes=[
            *[pltpu.VMEM((w.shape[0] * peers, w.shape[1]), bf16) for w in weights],
            pltpu.VMEM((tokens, query_rank), bf16),
            pltpu.VMEM((spread, tokens, pair_rank), bf16),
            pltpu.VMEM((spread, tokens, ROTARY), bf16),
            pltpu.VMEM((1, query_rank), f32),
            pltpu.VMEM((1, pair_rank), f32),
            pltpu.VMEM((3, tokens, narrow_query.shape[1]), f32),
            pltpu.VMEM((3, tokens, broad_query.shape[1]), f32),
            pltpu.VMEM(ktab.shape, f32),
            pltpu.VMEM((length, pair_rank), bf16),
            pltpu.VMEM((length, ROTARY), bf16),
            pltpu.SemaphoreType.DMA((7, KINDS)),
            pltpu.SemaphoreType.DMA((7, KINDS)),
            pltpu.SemaphoreType.DMA((2, spread, 3)),
            pltpu.SemaphoreType.DMA((spread, 3)),
            pltpu.SemaphoreType.DMA((6,)),
            pltpu.SemaphoreType.DMA((6,)),
        ],
        compiler_params=pltpu.CompilerParams(
            collective_id=0, has_side_effects=True, vmem_limit_bytes=48 * 2**20
        ),
    )(*operands)


def solution(mesh):
    in_specs = (
        P("dp", "sp", None),
        P("dp", "sp", None),
        P("dp", "sp", None),
        P(),
        P(),
        P("dp", None),
        P("dp", None),
        P("dp", None),
        P("dp", None),
        P("dp", None),
        P("dp", None),
    )
    out_specs = (P("dp", "sp", None), P("dp", "sp", None))
    spread = mesh.shape["sp"]

    def choose(*arrays):
        rows = [a.shape[0] for a in arrays[5:]]
        fits = lax.axis_size("dp") == 2**3 and all(r % (2 * ROW_TILE) == 0 for r in rows)
        if fits:
            return fused_call(spread, *arrays)
        return on_device(*arrays)

    return jax.shard_map(
        choose, mesh=mesh, in_specs=in_specs, out_specs=out_specs, check_vma=False
    )
```

```python
import functools
import math

import jax
import jax.numpy as jnp
import numpy as np
from jax import lax
from jax.experimental import pallas as pl
from jax.experimental.pallas import tpu as pltpu
from jax.sharding import PartitionSpec as P

PLAIN_NARROW = 64
PLAIN_BROAD = 128
ROTARY = 32
VALUE_SIZE = 64


EPSILON = 1e-06
ROTARY_BASE = 10000.0


def normalize(latent, gain_row):
    values = latent.astype(jnp.float32)
    scaled = values * lax.rsqrt(jnp.mean(values * values, axis=-1, keepdims=True) + EPSILON)
    return (scaled * gain_row).astype(jnp.bfloat16)


def rotate(values, positions):
    halfway = ROTARY // 2
    frequency = ROTARY_BASE ** (-jnp.arange(halfway, dtype=jnp.float32) / halfway)
    angles = positions[:, None] * frequency[None, :]
    cosine = jnp.cos(angles)[:, None, :]
    sine_part = jnp.sin(angles)[:, None, :]
    width = values.shape[-1]
    plain_part = values[..., : width - ROTARY]
    first_half = values[..., width - ROTARY : width - halfway]
    second_half = values[..., width - halfway :]
    return jnp.concatenate(
        [
            plain_part,
            first_half * cosine - second_half * sine_part,
            first_half * sine_part + second_half * cosine,
        ],
        axis=-1,
    )


def make_fold(latent, pieces):
    return tuple(
        (jnp.dot(latent, weight_rows, preferred_element_type=jnp.float32) for weight_rows in pieces)
    )


def arrange(sums, width, positions, groups, with_rotary):
    row_count = positions.shape[0]
    shaped = sums.reshape(row_count, -1, width)
    if with_rotary:
        shaped = rotate(shaped, positions)
    shaped = shaped.astype(jnp.bfloat16)
    return shaped.reshape(row_count, groups, shaped.shape[1] // groups, width)


def attend_group(queries, keys_plain, values, rope_keys, factor):
    length = queries.shape[0]
    block_rows = 512
    key_whole = jnp.concatenate([keys_plain[:, 0, :], rope_keys], axis=1)
    value_head = values[:, 0, :]

    def one_block(query_block):
        scores = (
            jnp.einsum("qd,kd->qk", query_block, key_whole, preferred_element_type=jnp.float32)
            * factor
        )
        shifted = jnp.exp(scores - jnp.max(scores, axis=-1, keepdims=True))
        totals = jnp.sum(shifted, axis=-1, keepdims=True)
        mixed = jnp.dot(
            shifted.astype(jnp.bfloat16), value_head, preferred_element_type=jnp.float32
        )
        return (mixed / totals).astype(jnp.bfloat16)

    blocks = lax.map(one_block, queries[:, 0, :].reshape(length // block_rows, block_rows, -1))
    results = [blocks.reshape(length, -1)]
    return jnp.stack(results, axis=1)


def attend_both(members, rope_keys):
    query_first, key_first, value_first, query_second, key_second, value_second = members
    mixed_first = attend_group(
        query_first[:, 0],
        key_first[:, 0],
        value_first[:, 0],
        rope_keys,
        (PLAIN_NARROW + ROTARY) ** (-0.5),
    )
    mixed_second = attend_group(
        query_second[:, 0],
        key_second[:, 0],
        value_second[:, 0],
        rope_keys,
        (PLAIN_BROAD + ROTARY) ** (-0.5),
    )
    return (mixed_first[:, None], mixed_second[:, None])


def finish(mixed):
    flattened = mixed.reshape(mixed.shape[0], -1).astype(jnp.float32)
    scaled = flattened * lax.rsqrt(
        jnp.mean(flattened * flattened, axis=-1, keepdims=True) + EPSILON
    )
    return scaled.astype(jnp.bfloat16)[None]


def on_device(
    query_latent,
    keyvalue_latent,
    rope_key,
    query_gain,
    keyvalue_gain,
    narrow_query,
    broad_query,
    narrow_key,
    narrow_value,
    broad_key,
    broad_value,
):
    tokens = query_latent.shape[1]
    spread = lax.axis_size("sp")
    device_index = lax.axis_index("sp")
    width_narrow = PLAIN_NARROW + ROTARY
    width_broad = PLAIN_BROAD + ROTARY
    query_normed = normalize(query_latent[0], query_gain)
    pair_normed = normalize(keyvalue_latent[0], keyvalue_gain)
    own_positions = (device_index * tokens + jnp.arange(tokens, dtype=jnp.int32)).astype(
        jnp.float32
    )
    rope_own = rotate(rope_key[0].astype(jnp.float32)[:, None, :], own_positions)[:, 0, :].astype(
        jnp.bfloat16
    )
    query_all, pair_all, rope_all = (
        lax.all_gather(query_normed, "sp", axis=0, tiled=True),
        lax.all_gather(pair_normed, "sp", axis=0, tiled=True),
        lax.all_gather(rope_own, "sp", axis=0, tiled=True),
    )
    length = tokens * spread
    all_positions = jnp.arange(length, dtype=jnp.int32).astype(jnp.float32)

    def own_columns(weight, width):
        count = weight.shape[1] // (width * spread)
        return lax.dynamic_slice_in_dim(weight, device_index * count * width, count * width, 1)

    own_narrow_query = own_columns(narrow_query, width_narrow)
    own_broad_query = own_columns(broad_query, width_broad)
    own_narrow_key = own_columns(narrow_key, PLAIN_NARROW)
    own_narrow_value = own_columns(narrow_value, VALUE_SIZE)
    own_broad_key = own_columns(broad_key, PLAIN_BROAD)
    own_broad_value = own_columns(broad_value, VALUE_SIZE)
    query_sums = make_fold(
        query_all,
        (
            lax.all_gather(own_narrow_query, "dp", axis=0, tiled=True),
            lax.all_gather(own_broad_query, "dp", axis=0, tiled=True),
        ),
    )
    pair_sums = make_fold(
        pair_all,
        (
            lax.all_gather(own_narrow_key, "dp", axis=0, tiled=True),
            lax.all_gather(own_narrow_value, "dp", axis=0, tiled=True),
            lax.all_gather(own_broad_key, "dp", axis=0, tiled=True),
            lax.all_gather(own_broad_value, "dp", axis=0, tiled=True),
        ),
    )
    members = (
        arrange(query_sums[0], width_narrow, all_positions, 1, True),
        arrange(pair_sums[0], PLAIN_NARROW, all_positions, 1, False),
        arrange(pair_sums[1], VALUE_SIZE, all_positions, 1, False),
        arrange(query_sums[1], width_broad, all_positions, 1, True),
        arrange(pair_sums[2], PLAIN_BROAD, all_positions, 1, False),
        arrange(pair_sums[3], VALUE_SIZE, all_positions, 1, False),
    )
    mixed_first, mixed_second = attend_both(members, rope_all)
    back_first, back_second = (
        lax.all_to_all(mixed_first, "sp", split_axis=0, concat_axis=1, tiled=True),
        lax.all_to_all(mixed_second, "sp", split_axis=0, concat_axis=1, tiled=True),
    )
    return (finish(back_first), finish(back_second))


MESH = pl.DeviceIdType.MESH
ROW_TILE = 16
LANES = 128
NK, NV, BK, BV, NQ, BQ = range(6)
KINDS = 9


def rotary_tables(length):
    halfway = ROTARY // 2
    frequency = (
        np.float32(ROTARY_BASE) ** (-np.arange(halfway, dtype=np.float32) / np.float32(halfway))
    ).astype(np.float32)
    angles = np.arange(length, dtype=np.float32)[:, None] * frequency[None, :]
    cosine = np.cos(angles.astype(np.float64)).astype(np.float32)
    sine = np.sin(angles.astype(np.float64)).astype(np.float32)
    return cosine, sine


def key_table(length):
    cosine, sine = rotary_tables(length)
    return np.concatenate([cosine, cosine, -sine, sine], 1)


def wide_tables(table, plain, heads):
    rows, halfway = table.shape[0], ROTARY // 2
    ones = jnp.ones((rows, plain), jnp.float32)
    zeros = jnp.zeros((rows, plain), jnp.float32)
    zero = jnp.zeros((rows, halfway), jnp.float32)
    keep = [ones, table[:, :ROTARY]]
    ahead = [zeros, table[:, ROTARY : ROTARY + halfway], zero]
    behind = [zeros, zero, table[:, ROTARY + halfway :]]
    return [jnp.concatenate(parts * heads, axis=1) for parts in (keep, ahead, behind)]


def fused(
    spread,
    heads,
    query_hbm,
    pair_hbm,
    rope_hbm,
    qgain_hbm,
    pgain_hbm,
    w0,
    w1,
    w2,
    w3,
    w4,
    w5,
    ktab_hbm,
    narrow_out,
    broad_out,
    g0,
    g1,
    g2,
    g3,
    g4,
    g5,
    query_buf,
    pair_buf,
    rope_buf,
    qgain,
    pgain,
    ntab,
    btab,
    ktab,
    pair_normed,
    rope_keys,
    send_sem,
    recv_sem,
    zsend_sem,
    zrecv_sem,
    local_sem,
    wlocal_sem,
):
    weights = (w0, w1, w2, w3, w4, w5)
    gathered = (g0, g1, g2, g3, g4, g5)
    tokens = query_hbm.shape[1]
    z = lax.axis_index("sp")
    me = lax.axis_index("dp")
    core = me % 2
    flip_p = 1 - 2 * core
    flip_x = 2 * (1 - 2 * ((me // 2) % 2))
    flip_y = 4 * (1 - 2 * (me // 4))
    peer_p, peer_x, peer_y = me + flip_p, me + flip_x, me + flip_y
    diagonal = me + flip_x + flip_y

    columns_all = [w.shape[1] for w in weights]
    pieces = [(a, 0, columns_all[a]) for a in (NK, NV, BK, BV, NQ)]
    split = -(-(columns_all[BQ] // 2) // LANES) * LANES
    pieces += [(BQ, 0, split), (BQ, split, columns_all[BQ] - split)]

    local = [
        pltpu.make_async_copy(pair_hbm.at[0], pair_buf.at[z], local_sem.at[0]),
        pltpu.make_async_copy(rope_hbm.at[0], rope_buf.at[z], local_sem.at[1]),
        pltpu.make_async_copy(query_hbm.at[0], query_buf, local_sem.at[2]),
        pltpu.make_async_copy(qgain_hbm, qgain.at[0], local_sem.at[3]),
        pltpu.make_async_copy(pgain_hbm, pgain.at[0], local_sem.at[4]),
        pltpu.make_async_copy(ktab_hbm, ktab, local_sem.at[5]),
    ]

    def rows_of(array, owner, half=None):
        rows = weights[array].shape[0]
        if half is None:
            return pl.ds(pl.multiple_of(owner * rows, rows), rows)
        part = rows // 2
        return pl.ds(pl.multiple_of(owner * rows + half * part, part), part)

    own_weights = [
        pltpu.make_async_copy(
            weights[a], gathered[a].at[rows_of(a, me)], wlocal_sem.at[a]
        )
        for a in range(len(weights))
    ]
    for copy in local + own_weights:
        copy.start()

    barrier = pltpu.get_barrier_semaphore()
    for peer in (peer_p, peer_x, peer_y):
        pl.semaphore_signal(barrier, inc=1, device_id=(z, peer), device_id_type=MESH)

    @pl.when(z > 0)
    def _():
        pl.semaphore_signal(barrier, inc=1, device_id=(z - 1, me), device_id_type=MESH)

    @pl.when(z < spread - 1)
    def _():
        pl.semaphore_signal(barrier, inc=1, device_id=(z + 1, me), device_id_type=MESH)

    line = (z + spread - 1) // spread + (2 * spread - 2 - z) // spread
    pl.semaphore_wait(barrier, 3 + line)

    chunks = 2
    chunk_rows = tokens // chunks

    def along(item, owner, step, own):
        if item < chunks:
            rows = pl.ds(item * chunk_rows, chunk_rows)
            target = pair_buf.at[owner, rows]
            source = pair_hbm.at[0, rows] if own else target
        else:
            target = rope_buf.at[owner]
            source = rope_hbm.at[0] if own else target
        return pltpu.make_async_remote_copy(
            src_ref=source,
            dst_ref=target,
            send_sem=zsend_sem.at[0 if step < 0 else 1, owner, item],
            recv_sem=zrecv_sem.at[owner, item],
            device_id=(z + step, me),
            device_id_type=MESH,
        )

    def send_along(owner, own, step, item):
        @pl.when((z > 0) if step < 0 else (z < spread - 1))
        def _():
            along(item, owner, step, own).start()

    items = range(chunks + 1)
    for item in items:
        for step in (-1, 1):
            send_along(z, True, step, item)

    def relay_along(distance, item):
        for side in (1, -1):
            owner = z + side * distance

            @pl.when((owner >= 0) & (owner < spread))
            def _():
                along(item, owner, -side, False).wait_recv()
                send_along(owner, False, -side, item)

    def across(index, kind):
        a, start, width = pieces[index]
        cols = pl.ds(start, width)
        target_of = {
            0: (me, None, peer_p),
            1: (me, None, peer_x),
            2: (me, None, peer_y),
            3: (peer_x, None, peer_p),
            4: (peer_y, None, peer_p),
            5: (peer_x, 0, peer_y),
            6: (peer_y, 1, peer_x),
            7: (diagonal, 0, peer_p),
            8: (diagonal, 1, peer_p),
        }
        owner, half, device = target_of[kind]
        target = gathered[a].at[rows_of(a, owner, half), cols]
        source = weights[a].at[:, cols] if kind < 3 else target
        return pltpu.make_async_remote_copy(
            src_ref=source,
            dst_ref=target,
            send_sem=send_sem.at[index, kind],
            recv_sem=recv_sem.at[index, kind],
            device_id=(z, device),
            device_id_type=MESH,
        )

    def arrived(index, kind):
        a, start, width = pieces[index]
        owner, half = {
            0: (peer_p, None),
            1: (peer_x, None),
            2: (peer_y, None),
            3: (peer_x + flip_p, None),
            4: (peer_y + flip_p, None),
            5: (diagonal, 0),
            6: (diagonal, 1),
            7: (diagonal + flip_p, 0),
            8: (diagonal + flip_p, 1),
        }[kind]
        target = gathered[a].at[rows_of(a, owner, half), pl.ds(start, width)]
        pltpu.make_async_remote_copy(
            src_ref=target,
            dst_ref=target,
            send_sem=send_sem.at[index, kind],
            recv_sem=recv_sem.at[index, kind],
            device_id=(z, peer_p),
            device_id_type=MESH,
        ).wait_recv()

    def send_own(index):
        for kind in (1, 2, 0):
            across(index, kind).start()

    def relay(index):
        arrived(index, 1)
        across(index, 5).start()
        across(index, 3).start()
        arrived(index, 2)
        across(index, 6).start()
        across(index, 4).start()

    def hand_over(index):
        for half in (0, 1):
            arrived(index, 5 + half)
            across(index, 7 + half).start()

    def complete(index):
        for kind in (0, 3, 4, 7, 8):
            arrived(index, kind)

    for index in range(4):
        send_own(index)

    def normed(values, gain):
        values = values.astype(jnp.float32)
        scaled = values * lax.rsqrt(jnp.mean(values * values, axis=-1, keepdims=True) + EPSILON)
        return (scaled * gain).astype(jnp.bfloat16)

    for copy in local:
        copy.wait()
    for copy in own_weights:
        copy.wait()
    query_normed = normed(query_buf[...], qgain[...])
    own_table = ktab[pl.ds(pl.multiple_of(z * tokens, tokens), tokens)]
    for table, plain in ((ntab, PLAIN_NARROW), (btab, PLAIN_BROAD)):
        for index, values in enumerate(wide_tables(own_table, plain, heads)):
            table[index] = values

    relay(0)
    send_own(4)
    for item in items:
        relay_along(1, item)
    relay(1)
    relay(2)
    relay(3)
    hand_over(0)
    send_own(5)
    send_own(6)
    hand_over(1)
    hand_over(2)
    for distance in range(2, spread):
        for item in items:
            relay_along(distance, item)
    hand_over(3)
    relay(4)
    relay(5)
    relay(6)
    for index in range(4):
        complete(index)

    for block in range(spread):
        rows = pl.ds(block * tokens, tokens)
        pair_normed[rows] = normed(pair_buf[block], pgain[...])
        plain = rope_buf[block].astype(jnp.float32).T
        halfway = ROTARY // 2
        swapped = jnp.concatenate([plain[:, halfway:], plain[:, :halfway]], axis=1)
        rope_keys[rows] = (
            plain * ktab[rows, :ROTARY] + swapped * ktab[rows, ROTARY:]
        ).astype(jnp.bfloat16)

    def product(left, right):
        return jnp.dot(left, right, preferred_element_type=jnp.float32)

    narrow_keys = product(pair_normed[...], g0[...]).astype(jnp.bfloat16)
    narrow_values = product(pair_normed[...], g1[...]).astype(jnp.bfloat16)
    hand_over(4)
    broad_keys = product(pair_normed[...], g2[...]).astype(jnp.bfloat16)
    broad_values = product(pair_normed[...], g3[...]).astype(jnp.bfloat16)
    hand_over(5)
    hand_over(6)

    def attend(query_weights, table, keys, values, plain, out):
        width = plain + ROTARY
        sums = product(query_normed, query_weights[...])
        total = sums.shape[1]
        halfway = ROTARY // 2
        queries = (
            sums * table[0]
            + pltpu.roll(sums, total - halfway, 1) * table[1]
            + pltpu.roll(sums, halfway, 1) * table[2]
        ).astype(jnp.bfloat16)
        factor = width ** (-0.5) * math.log2(math.e)
        attended = []
        for head in range(heads):
            query = queries[:, head * width : (head + 1) * width]
            key = jnp.concatenate(
                [keys[:, head * plain : (head + 1) * plain], rope_keys[...]], axis=1
            )
            scores = lax.dot_general(
                query, key, (((1,), (1,)), ((), ())), preferred_element_type=jnp.float32
            )
            shifted = jnp.exp2((scores - jnp.max(scores, axis=-1, keepdims=True)) * factor)
            totals = jnp.sum(shifted, axis=-1, keepdims=True)
            mixed = product(
                shifted.astype(jnp.bfloat16), values[:, head * VALUE_SIZE : (head + 1) * VALUE_SIZE]
            )
            attended.append((mixed / totals).astype(jnp.bfloat16).astype(jnp.float32))
        flat = jnp.concatenate(attended, axis=1)
        scaled = flat * lax.rsqrt(jnp.mean(flat * flat, axis=-1, keepdims=True) + EPSILON)
        out[0] = scaled.astype(jnp.bfloat16)

    complete(4)
    attend(g4, ntab, narrow_keys, narrow_values, PLAIN_NARROW, narrow_out)
    complete(5)
    complete(6)
    attend(g5, btab, broad_keys, broad_values, PLAIN_BROAD, broad_out)

    for index in range(len(pieces)):
        for kind in range(KINDS):
            across(index, kind).wait_send()
    for item in items:
        for step in (-1, 1):
            for distance in range(spread):
                owner = z - step * distance

                @pl.when(
                    (owner >= 0)
                    & (owner < spread)
                    & ((z > 0) if step < 0 else (z < spread - 1))
                )
                def _():
                    along(item, owner, step, False).wait_send()


def fused_call(
    spread,
    query_latent,
    keyvalue_latent,
    rope_key,
    query_gain,
    keyvalue_gain,
    narrow_query,
    broad_query,
    narrow_key,
    narrow_value,
    broad_key,
    broad_value,
):
    tokens, query_rank = query_latent.shape[1:]
    pair_rank = keyvalue_latent.shape[2]
    length = tokens * spread
    heads = narrow_value.shape[1] // VALUE_SIZE
    weights = (narrow_key, narrow_value, broad_key, broad_value, narrow_query, broad_query)
    peers = lax.axis_size("dp")
    ktab = key_table(length)
    operands = (
        query_latent,
        keyvalue_latent,
        jnp.swapaxes(rope_key, 1, 2),
        query_gain,
        keyvalue_gain,
        *weights,
        jnp.asarray(ktab),
    )
    out = jax.ShapeDtypeStruct((1, tokens, heads * VALUE_SIZE), jnp.bfloat16)
    bf16, f32 = jnp.bfloat16, jnp.float32
    return pl.pallas_call(
        functools.partial(fused, spread, heads),
        out_shape=(out, out),
        in_specs=[pl.BlockSpec(memory_space=pltpu.HBM)] * len(operands),
        out_specs=[pl.BlockSpec(memory_space=pltpu.VMEM)] * 2,
        scratch_shapes=[
            *[pltpu.VMEM((w.shape[0] * peers, w.shape[1]), bf16) for w in weights],
            pltpu.VMEM((tokens, query_rank), bf16),
            pltpu.VMEM((spread, tokens, pair_rank), bf16),
            pltpu.VMEM((spread, ROTARY, tokens), bf16),
            pltpu.VMEM((1, query_rank), f32),
            pltpu.VMEM((1, pair_rank), f32),
            pltpu.VMEM((3, tokens, narrow_query.shape[1]), f32),
            pltpu.VMEM((3, tokens, broad_query.shape[1]), f32),
            pltpu.VMEM(ktab.shape, f32),
            pltpu.VMEM((length, pair_rank), bf16),
            pltpu.VMEM((length, ROTARY), bf16),
            pltpu.SemaphoreType.DMA((7, KINDS)),
            pltpu.SemaphoreType.DMA((7, KINDS)),
            pltpu.SemaphoreType.DMA((2, spread, 3)),
            pltpu.SemaphoreType.DMA((spread, 3)),
            pltpu.SemaphoreType.DMA((6,)),
            pltpu.SemaphoreType.DMA((6,)),
        ],
        compiler_params=pltpu.CompilerParams(
            collective_id=0, has_side_effects=True, vmem_limit_bytes=60 * 2**20
        ),
    )(*operands)


def solution(mesh):
    in_specs = (
        P("dp", "sp", None),
        P("dp", "sp", None),
        P("dp", "sp", None),
        P(),
        P(),
        P("dp", None),
        P("dp", None),
        P("dp", None),
        P("dp", None),
        P("dp", None),
        P("dp", None),
    )
    out_specs = (P("dp", "sp", None), P("dp", "sp", None))
    spread = mesh.shape["sp"]

    def choose(*arrays):
        rows = [a.shape[0] for a in arrays[5:]]
        fits = lax.axis_size("dp") == 2**3 and all(r % (2 * ROW_TILE) == 0 for r in rows)
        if fits:
            return fused_call(spread, *arrays)
        return on_device(*arrays)

    return jax.shard_map(
        choose, mesh=mesh, in_specs=in_specs, out_specs=out_specs, check_vma=False
    )
```

```python
import functools
import math

import jax
import jax.numpy as jnp
import numpy as np
from jax import lax
from jax.experimental import pallas as pl
from jax.experimental.pallas import tpu as pltpu
from jax.sharding import PartitionSpec as P

PLAIN_NARROW = 64
PLAIN_BROAD = 128
ROTARY = 32
VALUE_SIZE = 64


EPSILON = 1e-06
ROTARY_BASE = 10000.0


def normalize(latent, gain_row):
    values = latent.astype(jnp.float32)
    scaled = values * lax.rsqrt(jnp.mean(values * values, axis=-1, keepdims=True) + EPSILON)
    return (scaled * gain_row).astype(jnp.bfloat16)


def rotate(values, positions):
    halfway = ROTARY // 2
    frequency = ROTARY_BASE ** (-jnp.arange(halfway, dtype=jnp.float32) / halfway)
    angles = positions[:, None] * frequency[None, :]
    cosine = jnp.cos(angles)[:, None, :]
    sine_part = jnp.sin(angles)[:, None, :]
    width = values.shape[-1]
    plain_part = values[..., : width - ROTARY]
    first_half = values[..., width - ROTARY : width - halfway]
    second_half = values[..., width - halfway :]
    return jnp.concatenate(
        [
            plain_part,
            first_half * cosine - second_half * sine_part,
            first_half * sine_part + second_half * cosine,
        ],
        axis=-1,
    )


def make_fold(latent, pieces):
    return tuple(
        (jnp.dot(latent, weight_rows, preferred_element_type=jnp.float32) for weight_rows in pieces)
    )


def arrange(sums, width, positions, groups, with_rotary):
    row_count = positions.shape[0]
    shaped = sums.reshape(row_count, -1, width)
    if with_rotary:
        shaped = rotate(shaped, positions)
    shaped = shaped.astype(jnp.bfloat16)
    return shaped.reshape(row_count, groups, shaped.shape[1] // groups, width)


def attend_group(queries, keys_plain, values, rope_keys, factor):
    length = queries.shape[0]
    block_rows = 512
    key_whole = jnp.concatenate([keys_plain[:, 0, :], rope_keys], axis=1)
    value_head = values[:, 0, :]

    def one_block(query_block):
        scores = (
            jnp.einsum("qd,kd->qk", query_block, key_whole, preferred_element_type=jnp.float32)
            * factor
        )
        shifted = jnp.exp(scores - jnp.max(scores, axis=-1, keepdims=True))
        totals = jnp.sum(shifted, axis=-1, keepdims=True)
        mixed = jnp.dot(
            shifted.astype(jnp.bfloat16), value_head, preferred_element_type=jnp.float32
        )
        return (mixed / totals).astype(jnp.bfloat16)

    blocks = lax.map(one_block, queries[:, 0, :].reshape(length // block_rows, block_rows, -1))
    results = [blocks.reshape(length, -1)]
    return jnp.stack(results, axis=1)


def attend_both(members, rope_keys):
    query_first, key_first, value_first, query_second, key_second, value_second = members
    mixed_first = attend_group(
        query_first[:, 0],
        key_first[:, 0],
        value_first[:, 0],
        rope_keys,
        (PLAIN_NARROW + ROTARY) ** (-0.5),
    )
    mixed_second = attend_group(
        query_second[:, 0],
        key_second[:, 0],
        value_second[:, 0],
        rope_keys,
        (PLAIN_BROAD + ROTARY) ** (-0.5),
    )
    return (mixed_first[:, None], mixed_second[:, None])


def finish(mixed):
    flattened = mixed.reshape(mixed.shape[0], -1).astype(jnp.float32)
    scaled = flattened * lax.rsqrt(
        jnp.mean(flattened * flattened, axis=-1, keepdims=True) + EPSILON
    )
    return scaled.astype(jnp.bfloat16)[None]


def on_device(
    query_latent,
    keyvalue_latent,
    rope_key,
    query_gain,
    keyvalue_gain,
    narrow_query,
    broad_query,
    narrow_key,
    narrow_value,
    broad_key,
    broad_value,
):
    tokens = query_latent.shape[1]
    spread = lax.axis_size("sp")
    device_index = lax.axis_index("sp")
    width_narrow = PLAIN_NARROW + ROTARY
    width_broad = PLAIN_BROAD + ROTARY
    query_normed = normalize(query_latent[0], query_gain)
    pair_normed = normalize(keyvalue_latent[0], keyvalue_gain)
    own_positions = (device_index * tokens + jnp.arange(tokens, dtype=jnp.int32)).astype(
        jnp.float32
    )
    rope_own = rotate(rope_key[0].astype(jnp.float32)[:, None, :], own_positions)[:, 0, :].astype(
        jnp.bfloat16
    )
    query_all, pair_all, rope_all = (
        lax.all_gather(query_normed, "sp", axis=0, tiled=True),
        lax.all_gather(pair_normed, "sp", axis=0, tiled=True),
        lax.all_gather(rope_own, "sp", axis=0, tiled=True),
    )
    length = tokens * spread
    all_positions = jnp.arange(length, dtype=jnp.int32).astype(jnp.float32)

    def own_columns(weight, width):
        count = weight.shape[1] // (width * spread)
        return lax.dynamic_slice_in_dim(weight, device_index * count * width, count * width, 1)

    own_narrow_query = own_columns(narrow_query, width_narrow)
    own_broad_query = own_columns(broad_query, width_broad)
    own_narrow_key = own_columns(narrow_key, PLAIN_NARROW)
    own_narrow_value = own_columns(narrow_value, VALUE_SIZE)
    own_broad_key = own_columns(broad_key, PLAIN_BROAD)
    own_broad_value = own_columns(broad_value, VALUE_SIZE)
    query_sums = make_fold(
        query_all,
        (
            lax.all_gather(own_narrow_query, "dp", axis=0, tiled=True),
            lax.all_gather(own_broad_query, "dp", axis=0, tiled=True),
        ),
    )
    pair_sums = make_fold(
        pair_all,
        (
            lax.all_gather(own_narrow_key, "dp", axis=0, tiled=True),
            lax.all_gather(own_narrow_value, "dp", axis=0, tiled=True),
            lax.all_gather(own_broad_key, "dp", axis=0, tiled=True),
            lax.all_gather(own_broad_value, "dp", axis=0, tiled=True),
        ),
    )
    members = (
        arrange(query_sums[0], width_narrow, all_positions, 1, True),
        arrange(pair_sums[0], PLAIN_NARROW, all_positions, 1, False),
        arrange(pair_sums[1], VALUE_SIZE, all_positions, 1, False),
        arrange(query_sums[1], width_broad, all_positions, 1, True),
        arrange(pair_sums[2], PLAIN_BROAD, all_positions, 1, False),
        arrange(pair_sums[3], VALUE_SIZE, all_positions, 1, False),
    )
    mixed_first, mixed_second = attend_both(members, rope_all)
    back_first, back_second = (
        lax.all_to_all(mixed_first, "sp", split_axis=0, concat_axis=1, tiled=True),
        lax.all_to_all(mixed_second, "sp", split_axis=0, concat_axis=1, tiled=True),
    )
    return (finish(back_first), finish(back_second))


MESH = pl.DeviceIdType.MESH
ROW_TILE = 16
LANES = 128
NK, NV, NQ, BK, BV, BQ = range(6)
KINDS = 9


def rotary_tables(length):
    halfway = ROTARY // 2
    frequency = (
        np.float32(ROTARY_BASE) ** (-np.arange(halfway, dtype=np.float32) / np.float32(halfway))
    ).astype(np.float32)
    angles = np.arange(length, dtype=np.float32)[:, None] * frequency[None, :]
    cosine = np.cos(angles.astype(np.float64)).astype(np.float32)
    sine = np.sin(angles.astype(np.float64)).astype(np.float32)
    return cosine, sine


def key_table(length):
    cosine, sine = rotary_tables(length)
    return np.concatenate([cosine, cosine, -sine, sine], 1)


def wide_tables(table, plain, heads):
    rows, halfway = table.shape[0], ROTARY // 2
    ones = jnp.ones((rows, plain), jnp.float32)
    zeros = jnp.zeros((rows, plain), jnp.float32)
    zero = jnp.zeros((rows, halfway), jnp.float32)
    keep = [ones, table[:, :ROTARY]]
    ahead = [zeros, table[:, ROTARY : ROTARY + halfway], zero]
    behind = [zeros, zero, table[:, ROTARY + halfway :]]
    return [jnp.concatenate(parts * heads, axis=1) for parts in (keep, ahead, behind)]


def fused(
    spread,
    heads,
    query_hbm,
    pair_hbm,
    rope_hbm,
    qgain_hbm,
    pgain_hbm,
    w0,
    w1,
    w2,
    w3,
    w4,
    w5,
    ktab_hbm,
    narrow_out,
    broad_out,
    g0,
    g1,
    g2,
    g3,
    g4,
    g5,
    query_buf,
    pair_buf,
    rope_buf,
    qgain,
    pgain,
    ntab,
    btab,
    ktab,
    pair_normed,
    rope_keys,
    narrow_sums,
    broad_sums,
    send_sem,
    recv_sem,
    zsend_sem,
    zrecv_sem,
    local_sem,
    wlocal_sem,
):
    weights = (w0, w1, w2, w3, w4, w5)
    gathered = (g0, g1, g2, g3, g4, g5)
    tokens = query_hbm.shape[1]
    z = lax.axis_index("sp")
    me = lax.axis_index("dp")
    core = me % 2
    flip_p = 1 - 2 * core
    flip_x = 2 * (1 - 2 * ((me // 2) % 2))
    flip_y = 4 * (1 - 2 * (me // 4))
    peer_p, peer_x, peer_y = me + flip_p, me + flip_x, me + flip_y
    diagonal = me + flip_x + flip_y

    columns_all = [w.shape[1] for w in weights]
    pieces = [(a, 0, columns_all[a]) for a in (NK, NV, NQ, BK, BV)]
    split = -(-(columns_all[BQ] // 2) // LANES) * LANES
    pieces += [(BQ, 0, split), (BQ, split, columns_all[BQ] - split)]

    local = [
        pltpu.make_async_copy(pair_hbm.at[0], pair_buf.at[z], local_sem.at[0]),
        pltpu.make_async_copy(rope_hbm.at[0], rope_buf.at[z], local_sem.at[1]),
        pltpu.make_async_copy(query_hbm.at[0], query_buf, local_sem.at[2]),
        pltpu.make_async_copy(qgain_hbm, qgain.at[0], local_sem.at[3]),
        pltpu.make_async_copy(pgain_hbm, pgain.at[0], local_sem.at[4]),
        pltpu.make_async_copy(ktab_hbm, ktab, local_sem.at[5]),
    ]

    def rows_of(array, owner, half=None):
        rows = weights[array].shape[0]
        if half is None:
            return pl.ds(pl.multiple_of(owner * rows, rows), rows)
        part = rows // 2
        return pl.ds(pl.multiple_of(owner * rows + half * part, part), part)

    own_weights = [
        pltpu.make_async_copy(
            weights[a], gathered[a].at[rows_of(a, me)], wlocal_sem.at[a]
        )
        for a in range(len(weights))
    ]
    for copy in local + own_weights:
        copy.start()

    barrier = pltpu.get_barrier_semaphore()
    for peer in (peer_p, peer_x, peer_y):
        pl.semaphore_signal(barrier, inc=1, device_id=(z, peer), device_id_type=MESH)

    @pl.when(z > 0)
    def _():
        pl.semaphore_signal(barrier, inc=1, device_id=(z - 1, me), device_id_type=MESH)

    @pl.when(z < spread - 1)
    def _():
        pl.semaphore_signal(barrier, inc=1, device_id=(z + 1, me), device_id_type=MESH)

    line = (z + spread - 1) // spread + (2 * spread - 2 - z) // spread
    pl.semaphore_wait(barrier, 3 + line)

    chunks = 2
    chunk_rows = tokens // chunks

    def along(item, owner, step, own):
        if item < chunks:
            rows = pl.ds(item * chunk_rows, chunk_rows)
            target = pair_buf.at[owner, rows]
            source = pair_hbm.at[0, rows] if own else target
        else:
            target = rope_buf.at[owner]
            source = rope_hbm.at[0] if own else target
        return pltpu.make_async_remote_copy(
            src_ref=source,
            dst_ref=target,
            send_sem=zsend_sem.at[0 if step < 0 else 1, owner, item],
            recv_sem=zrecv_sem.at[owner, item],
            device_id=(z + step, me),
            device_id_type=MESH,
        )

    def send_along(owner, own, step, item):
        @pl.when((z > 0) if step < 0 else (z < spread - 1))
        def _():
            along(item, owner, step, own).start()

    items = range(chunks + 1)
    for item in items:
        for step in (-1, 1):
            send_along(z, True, step, item)

    def relay_along(distance, item):
        for side in (1, -1):
            owner = z + side * distance

            @pl.when((owner >= 0) & (owner < spread))
            def _():
                along(item, owner, -side, False).wait_recv()
                send_along(owner, False, -side, item)

    def across(index, kind):
        a, start, width = pieces[index]
        cols = pl.ds(start, width)
        target_of = {
            0: (me, None, peer_p),
            1: (me, None, peer_x),
            2: (me, None, peer_y),
            3: (peer_x, None, peer_p),
            4: (peer_y, None, peer_p),
            5: (peer_x, 0, peer_y),
            6: (peer_y, 1, peer_x),
            7: (diagonal, 0, peer_p),
            8: (diagonal, 1, peer_p),
        }
        owner, half, device = target_of[kind]
        target = gathered[a].at[rows_of(a, owner, half), cols]
        source = weights[a].at[:, cols] if kind < 3 else target
        return pltpu.make_async_remote_copy(
            src_ref=source,
            dst_ref=target,
            send_sem=send_sem.at[index, kind],
            recv_sem=recv_sem.at[index, kind],
            device_id=(z, device),
            device_id_type=MESH,
        )

    def arrived(index, kind):
        a, start, width = pieces[index]
        owner, half = {
            0: (peer_p, None),
            1: (peer_x, None),
            2: (peer_y, None),
            3: (peer_x + flip_p, None),
            4: (peer_y + flip_p, None),
            5: (diagonal, 0),
            6: (diagonal, 1),
            7: (diagonal + flip_p, 0),
            8: (diagonal + flip_p, 1),
        }[kind]
        target = gathered[a].at[rows_of(a, owner, half), pl.ds(start, width)]
        pltpu.make_async_remote_copy(
            src_ref=target,
            dst_ref=target,
            send_sem=send_sem.at[index, kind],
            recv_sem=recv_sem.at[index, kind],
            device_id=(z, peer_p),
            device_id_type=MESH,
        ).wait_recv()

    def send_own(index):
        for kind in (1, 2, 0):
            across(index, kind).start()

    def relay(index):
        arrived(index, 1)
        across(index, 5).start()
        across(index, 3).start()
        arrived(index, 2)
        across(index, 6).start()
        across(index, 4).start()

    def hand_over(index):
        for half in (0, 1):
            arrived(index, 5 + half)
            across(index, 7 + half).start()

    def complete(index):
        for kind in (0, 3, 4, 7, 8):
            arrived(index, kind)

    for index in range(4):
        send_own(index)

    def normed(values, gain):
        values = values.astype(jnp.float32)
        scaled = values * lax.rsqrt(jnp.mean(values * values, axis=-1, keepdims=True) + EPSILON)
        return (scaled * gain).astype(jnp.bfloat16)

    for copy in local:
        copy.wait()
    for copy in own_weights:
        copy.wait()
    query_normed = normed(query_buf[...], qgain[...])
    own_table = ktab[pl.ds(pl.multiple_of(z * tokens, tokens), tokens)]
    for table, plain in ((ntab, PLAIN_NARROW), (btab, PLAIN_BROAD)):
        for index, values in enumerate(wide_tables(own_table, plain, heads)):
            table[index] = values

    relay(0)
    send_own(4)
    relay(1)
    for item in items:
        relay_along(1, item)
    relay(2)
    relay(3)
    send_own(5)
    send_own(6)
    hand_over(0)
    hand_over(1)
    for item in items:
        relay_along(2, item)
    relay(4)
    hand_over(2)
    for distance in range(3, spread):
        for item in items:
            relay_along(distance, item)
    hand_over(3)
    relay(5)
    for index in range(3):
        complete(index)

    for block in range(spread):
        rows = pl.ds(block * tokens, tokens)
        pair_normed[rows] = normed(pair_buf[block], pgain[...])
        plain = rope_buf[block].astype(jnp.float32).T
        halfway = ROTARY // 2
        swapped = jnp.concatenate([plain[:, halfway:], plain[:, :halfway]], axis=1)
        rope_keys[rows] = (
            plain * ktab[rows, :ROTARY] + swapped * ktab[rows, ROTARY:]
        ).astype(jnp.bfloat16)

    def product(left, right):
        return jnp.dot(left, right, preferred_element_type=jnp.float32)

    def project(sums, array, start, width):
        cols = pl.ds(start, width)
        sums[:, cols] = product(query_normed, gathered[array][:, cols])

    def rotated(sums, table, start, stop):
        halfway, cols = ROTARY // 2, pl.ds(start, stop - start)
        values = sums[:, cols]
        return (
            values * table[0, :, cols]
            + pltpu.roll(values, stop - start - halfway, 1) * table[1, :, cols]
            + pltpu.roll(values, halfway, 1) * table[2, :, cols]
        ).astype(jnp.bfloat16)

    def attend(queries, start, keys, values, plain, which):
        width = plain + ROTARY
        factor = width ** (-0.5) * math.log2(math.e)
        attended = []
        for head in which:
            query = queries[:, head * width - start : (head + 1) * width - start]
            key = jnp.concatenate(
                [keys[:, head * plain : (head + 1) * plain], rope_keys[...]], axis=1
            )
            scores = lax.dot_general(
                query, key, (((1,), (1,)), ((), ())), preferred_element_type=jnp.float32
            )
            shifted = jnp.exp2((scores - jnp.max(scores, axis=-1, keepdims=True)) * factor)
            totals = jnp.sum(shifted, axis=-1, keepdims=True)
            mixed = product(
                shifted.astype(jnp.bfloat16), values[:, head * VALUE_SIZE : (head + 1) * VALUE_SIZE]
            )
            attended.append((mixed / totals).astype(jnp.bfloat16).astype(jnp.float32))
        return attended

    def finish_group(attended, out):
        flat = jnp.concatenate(attended, axis=1)
        scaled = flat * lax.rsqrt(jnp.mean(flat * flat, axis=-1, keepdims=True) + EPSILON)
        out[0] = scaled.astype(jnp.bfloat16)

    project(narrow_sums, NQ, 0, columns_all[NQ])
    narrow_queries = rotated(narrow_sums, ntab, 0, columns_all[NQ])
    narrow_keys = product(pair_normed[...], gathered[NK][...]).astype(jnp.bfloat16)
    narrow_values = product(pair_normed[...], gathered[NV][...]).astype(jnp.bfloat16)
    relay(6)
    hand_over(4)
    complete(3)
    broad_keys = product(pair_normed[...], gathered[BK][...]).astype(jnp.bfloat16)
    hand_over(5)
    finish_group(
        attend(narrow_queries, 0, narrow_keys, narrow_values, PLAIN_NARROW, range(heads)),
        narrow_out,
    )
    hand_over(6)
    complete(4)
    broad_values = product(pair_normed[...], gathered[BV][...]).astype(jnp.bfloat16)
    complete(5)
    width_broad = PLAIN_BROAD + ROTARY
    early = split // width_broad
    project(broad_sums, BQ, 0, split)
    attended = attend(
        rotated(broad_sums, btab, 0, split), 0, broad_keys, broad_values, PLAIN_BROAD, range(early)
    )
    complete(6)
    project(broad_sums, BQ, split, columns_all[BQ] - split)
    start = early * width_broad // LANES * LANES
    attended += attend(
        rotated(broad_sums, btab, start, columns_all[BQ]),
        start,
        broad_keys,
        broad_values,
        PLAIN_BROAD,
        range(early, heads),
    )
    finish_group(attended, broad_out)

    for index in range(len(pieces)):
        for kind in range(KINDS):
            across(index, kind).wait_send()
    for item in items:
        for step in (-1, 1):
            for distance in range(spread):
                owner = z - step * distance

                @pl.when(
                    (owner >= 0)
                    & (owner < spread)
                    & ((z > 0) if step < 0 else (z < spread - 1))
                )
                def _():
                    along(item, owner, step, False).wait_send()


def fused_call(
    spread,
    query_latent,
    keyvalue_latent,
    rope_key,
    query_gain,
    keyvalue_gain,
    narrow_query,
    broad_query,
    narrow_key,
    narrow_value,
    broad_key,
    broad_value,
):
    tokens, query_rank = query_latent.shape[1:]
    pair_rank = keyvalue_latent.shape[2]
    length = tokens * spread
    heads = narrow_value.shape[1] // VALUE_SIZE
    weights = (narrow_key, narrow_value, narrow_query, broad_key, broad_value, broad_query)
    peers = lax.axis_size("dp")
    ktab = key_table(length)
    operands = (
        query_latent,
        keyvalue_latent,
        jnp.swapaxes(rope_key, 1, 2),
        query_gain,
        keyvalue_gain,
        *weights,
        jnp.asarray(ktab),
    )
    out = jax.ShapeDtypeStruct((1, tokens, heads * VALUE_SIZE), jnp.bfloat16)
    bf16, f32 = jnp.bfloat16, jnp.float32
    return pl.pallas_call(
        functools.partial(fused, spread, heads),
        out_shape=(out, out),
        in_specs=[pl.BlockSpec(memory_space=pltpu.HBM)] * len(operands),
        out_specs=[pl.BlockSpec(memory_space=pltpu.VMEM)] * 2,
        scratch_shapes=[
            *[pltpu.VMEM((w.shape[0] * peers, w.shape[1]), bf16) for w in weights],
            pltpu.VMEM((tokens, query_rank), bf16),
            pltpu.VMEM((spread, tokens, pair_rank), bf16),
            pltpu.VMEM((spread, ROTARY, tokens), bf16),
            pltpu.VMEM((1, query_rank), f32),
            pltpu.VMEM((1, pair_rank), f32),
            pltpu.VMEM((3, tokens, narrow_query.shape[1]), f32),
            pltpu.VMEM((3, tokens, broad_query.shape[1]), f32),
            pltpu.VMEM(ktab.shape, f32),
            pltpu.VMEM((length, pair_rank), bf16),
            pltpu.VMEM((length, ROTARY), bf16),
            pltpu.VMEM((tokens, narrow_query.shape[1]), f32),
            pltpu.VMEM((tokens, broad_query.shape[1]), f32),
            pltpu.SemaphoreType.DMA((7, KINDS)),
            pltpu.SemaphoreType.DMA((7, KINDS)),
            pltpu.SemaphoreType.DMA((2, spread, 3)),
            pltpu.SemaphoreType.DMA((spread, 3)),
            pltpu.SemaphoreType.DMA((6,)),
            pltpu.SemaphoreType.DMA((6,)),
        ],
        compiler_params=pltpu.CompilerParams(
            collective_id=0, has_side_effects=True, vmem_limit_bytes=60 * 2**20
        ),
    )(*operands)


def solution(mesh):
    in_specs = (
        P("dp", "sp", None),
        P("dp", "sp", None),
        P("dp", "sp", None),
        P(),
        P(),
        P("dp", None),
        P("dp", None),
        P("dp", None),
        P("dp", None),
        P("dp", None),
        P("dp", None),
    )
    out_specs = (P("dp", "sp", None), P("dp", "sp", None))
    spread = mesh.shape["sp"]

    def choose(*arrays):
        rows = [a.shape[0] for a in arrays[5:]]
        fits = lax.axis_size("dp") == 2**3 and all(r % (2 * ROW_TILE) == 0 for r in rows)
        if fits:
            return fused_call(spread, *arrays)
        return on_device(*arrays)

    return jax.shard_map(
        choose, mesh=mesh, in_specs=in_specs, out_specs=out_specs, check_vma=False
    )
```

```python
import functools
import math

import jax
import jax.numpy as jnp
import numpy as np
from jax import lax
from jax.experimental import pallas as pl
from jax.experimental.pallas import tpu as pltpu
from jax.sharding import PartitionSpec as P

PLAIN_NARROW = 64
PLAIN_BROAD = 128
ROTARY = 32
VALUE_SIZE = 64


EPSILON = 1e-06
ROTARY_BASE = 10000.0


def normalize(latent, gain_row):
    values = latent.astype(jnp.float32)
    scaled = values * lax.rsqrt(jnp.mean(values * values, axis=-1, keepdims=True) + EPSILON)
    return (scaled * gain_row).astype(jnp.bfloat16)


def rotate(values, positions):
    halfway = ROTARY // 2
    frequency = ROTARY_BASE ** (-jnp.arange(halfway, dtype=jnp.float32) / halfway)
    angles = positions[:, None] * frequency[None, :]
    cosine = jnp.cos(angles)[:, None, :]
    sine_part = jnp.sin(angles)[:, None, :]
    width = values.shape[-1]
    plain_part = values[..., : width - ROTARY]
    first_half = values[..., width - ROTARY : width - halfway]
    second_half = values[..., width - halfway :]
    return jnp.concatenate(
        [
            plain_part,
            first_half * cosine - second_half * sine_part,
            first_half * sine_part + second_half * cosine,
        ],
        axis=-1,
    )


def make_fold(latent, pieces):
    return tuple(
        (jnp.dot(latent, weight_rows, preferred_element_type=jnp.float32) for weight_rows in pieces)
    )


def arrange(sums, width, positions, groups, with_rotary):
    row_count = positions.shape[0]
    shaped = sums.reshape(row_count, -1, width)
    if with_rotary:
        shaped = rotate(shaped, positions)
    shaped = shaped.astype(jnp.bfloat16)
    return shaped.reshape(row_count, groups, shaped.shape[1] // groups, width)


def attend_group(queries, keys_plain, values, rope_keys, factor):
    length = queries.shape[0]
    block_rows = 512
    key_whole = jnp.concatenate([keys_plain[:, 0, :], rope_keys], axis=1)
    value_head = values[:, 0, :]

    def one_block(query_block):
        scores = (
            jnp.einsum("qd,kd->qk", query_block, key_whole, preferred_element_type=jnp.float32)
            * factor
        )
        shifted = jnp.exp(scores - jnp.max(scores, axis=-1, keepdims=True))
        totals = jnp.sum(shifted, axis=-1, keepdims=True)
        mixed = jnp.dot(
            shifted.astype(jnp.bfloat16), value_head, preferred_element_type=jnp.float32
        )
        return (mixed / totals).astype(jnp.bfloat16)

    blocks = lax.map(one_block, queries[:, 0, :].reshape(length // block_rows, block_rows, -1))
    results = [blocks.reshape(length, -1)]
    return jnp.stack(results, axis=1)


def attend_both(members, rope_keys):
    query_first, key_first, value_first, query_second, key_second, value_second = members
    mixed_first = attend_group(
        query_first[:, 0],
        key_first[:, 0],
        value_first[:, 0],
        rope_keys,
        (PLAIN_NARROW + ROTARY) ** (-0.5),
    )
    mixed_second = attend_group(
        query_second[:, 0],
        key_second[:, 0],
        value_second[:, 0],
        rope_keys,
        (PLAIN_BROAD + ROTARY) ** (-0.5),
    )
    return (mixed_first[:, None], mixed_second[:, None])


def finish(mixed):
    flattened = mixed.reshape(mixed.shape[0], -1).astype(jnp.float32)
    scaled = flattened * lax.rsqrt(
        jnp.mean(flattened * flattened, axis=-1, keepdims=True) + EPSILON
    )
    return scaled.astype(jnp.bfloat16)[None]


def on_device(
    query_latent,
    keyvalue_latent,
    rope_key,
    query_gain,
    keyvalue_gain,
    narrow_query,
    broad_query,
    narrow_key,
    narrow_value,
    broad_key,
    broad_value,
):
    tokens = query_latent.shape[1]
    spread = lax.axis_size("sp")
    device_index = lax.axis_index("sp")
    width_narrow = PLAIN_NARROW + ROTARY
    width_broad = PLAIN_BROAD + ROTARY
    query_normed = normalize(query_latent[0], query_gain)
    pair_normed = normalize(keyvalue_latent[0], keyvalue_gain)
    own_positions = (device_index * tokens + jnp.arange(tokens, dtype=jnp.int32)).astype(
        jnp.float32
    )
    rope_own = rotate(rope_key[0].astype(jnp.float32)[:, None, :], own_positions)[:, 0, :].astype(
        jnp.bfloat16
    )
    query_all, pair_all, rope_all = (
        lax.all_gather(query_normed, "sp", axis=0, tiled=True),
        lax.all_gather(pair_normed, "sp", axis=0, tiled=True),
        lax.all_gather(rope_own, "sp", axis=0, tiled=True),
    )
    length = tokens * spread
    all_positions = jnp.arange(length, dtype=jnp.int32).astype(jnp.float32)

    def own_columns(weight, width):
        count = weight.shape[1] // (width * spread)
        return lax.dynamic_slice_in_dim(weight, device_index * count * width, count * width, 1)

    own_narrow_query = own_columns(narrow_query, width_narrow)
    own_broad_query = own_columns(broad_query, width_broad)
    own_narrow_key = own_columns(narrow_key, PLAIN_NARROW)
    own_narrow_value = own_columns(narrow_value, VALUE_SIZE)
    own_broad_key = own_columns(broad_key, PLAIN_BROAD)
    own_broad_value = own_columns(broad_value, VALUE_SIZE)
    query_sums = make_fold(
        query_all,
        (
            lax.all_gather(own_narrow_query, "dp", axis=0, tiled=True),
            lax.all_gather(own_broad_query, "dp", axis=0, tiled=True),
        ),
    )
    pair_sums = make_fold(
        pair_all,
        (
            lax.all_gather(own_narrow_key, "dp", axis=0, tiled=True),
            lax.all_gather(own_narrow_value, "dp", axis=0, tiled=True),
            lax.all_gather(own_broad_key, "dp", axis=0, tiled=True),
            lax.all_gather(own_broad_value, "dp", axis=0, tiled=True),
        ),
    )
    members = (
        arrange(query_sums[0], width_narrow, all_positions, 1, True),
        arrange(pair_sums[0], PLAIN_NARROW, all_positions, 1, False),
        arrange(pair_sums[1], VALUE_SIZE, all_positions, 1, False),
        arrange(query_sums[1], width_broad, all_positions, 1, True),
        arrange(pair_sums[2], PLAIN_BROAD, all_positions, 1, False),
        arrange(pair_sums[3], VALUE_SIZE, all_positions, 1, False),
    )
    mixed_first, mixed_second = attend_both(members, rope_all)
    back_first, back_second = (
        lax.all_to_all(mixed_first, "sp", split_axis=0, concat_axis=1, tiled=True),
        lax.all_to_all(mixed_second, "sp", split_axis=0, concat_axis=1, tiled=True),
    )
    return (finish(back_first), finish(back_second))


MESH = pl.DeviceIdType.MESH
ROW_TILE = 16
LANES = 128
NK, NV, NQ, BK, BV, BQ = range(6)
KINDS = 9


def rotary_tables(length):
    halfway = ROTARY // 2
    frequency = (
        np.float32(ROTARY_BASE) ** (-np.arange(halfway, dtype=np.float32) / np.float32(halfway))
    ).astype(np.float32)
    angles = np.arange(length, dtype=np.float32)[:, None] * frequency[None, :]
    cosine = np.cos(angles.astype(np.float64)).astype(np.float32)
    sine = np.sin(angles.astype(np.float64)).astype(np.float32)
    return cosine, sine


def key_table(length):
    cosine, sine = rotary_tables(length)
    return np.concatenate([cosine, cosine, -sine, sine], 1)


def wide_tables(table, plain, heads):
    rows, halfway = table.shape[0], ROTARY // 2
    ones = jnp.ones((rows, plain), jnp.float32)
    zeros = jnp.zeros((rows, plain), jnp.float32)
    zero = jnp.zeros((rows, halfway), jnp.float32)
    keep = [ones, table[:, :ROTARY]]
    ahead = [zeros, table[:, ROTARY : ROTARY + halfway], zero]
    behind = [zeros, zero, table[:, ROTARY + halfway :]]
    return [jnp.concatenate(parts * heads, axis=1) for parts in (keep, ahead, behind)]


def fused(
    spread,
    heads,
    query_hbm,
    pair_hbm,
    rope_hbm,
    qgain_hbm,
    pgain_hbm,
    w0,
    w1,
    w2,
    w3,
    w4,
    w5,
    ktab_hbm,
    narrow_out,
    broad_out,
    g0,
    g1,
    g2,
    g3,
    g4,
    g5,
    query_buf,
    pair_buf,
    rope_buf,
    qgain,
    pgain,
    ntab,
    btab,
    ktab,
    pair_normed,
    rope_keys,
    narrow_sums,
    broad_sums,
    send_sem,
    recv_sem,
    zsend_sem,
    zrecv_sem,
    local_sem,
    wlocal_sem,
):
    weights = (w0, w1, w2, w3, w4, w5)
    gathered = (g0, g1, g2, g3, g4, g5)
    tokens = query_hbm.shape[1]
    z = lax.axis_index("sp")
    me = lax.axis_index("dp")
    core = me % 2
    flip_p = 1 - 2 * core
    flip_x = 2 * (1 - 2 * ((me // 2) % 2))
    flip_y = 4 * (1 - 2 * (me // 4))
    peer_p, peer_x, peer_y = me + flip_p, me + flip_x, me + flip_y
    diagonal = me + flip_x + flip_y

    columns_all = [w.shape[1] for w in weights]
    pieces = [(a, 0, columns_all[a]) for a in (NK, NV, NQ, BK, BV)]
    split = -(-(columns_all[BQ] // 2) // LANES) * LANES
    pieces += [(BQ, 0, split), (BQ, split, columns_all[BQ] - split)]

    local = [
        pltpu.make_async_copy(pair_hbm.at[0], pair_buf.at[z], local_sem.at[0]),
        pltpu.make_async_copy(rope_hbm.at[0], rope_buf.at[z], local_sem.at[1]),
        pltpu.make_async_copy(query_hbm.at[0], query_buf, local_sem.at[2]),
        pltpu.make_async_copy(qgain_hbm, qgain.at[0], local_sem.at[3]),
        pltpu.make_async_copy(pgain_hbm, pgain.at[0], local_sem.at[4]),
        pltpu.make_async_copy(ktab_hbm, ktab, local_sem.at[5]),
    ]

    def rows_of(array, owner, half=None):
        rows = weights[array].shape[0]
        if half is None:
            return pl.ds(pl.multiple_of(owner * rows, rows), rows)
        part = rows // 2
        return pl.ds(pl.multiple_of(owner * rows + half * part, part), part)

    own_weights = [
        pltpu.make_async_copy(
            weights[a], gathered[a].at[rows_of(a, me)], wlocal_sem.at[a]
        )
        for a in range(len(weights))
    ]
    for copy in local + own_weights:
        copy.start()

    barrier = pltpu.get_barrier_semaphore()
    for peer in (peer_p, peer_x, peer_y):
        pl.semaphore_signal(barrier, inc=1, device_id=(z, peer), device_id_type=MESH)

    @pl.when(z > 0)
    def _():
        pl.semaphore_signal(barrier, inc=1, device_id=(z - 1, me), device_id_type=MESH)

    @pl.when(z < spread - 1)
    def _():
        pl.semaphore_signal(barrier, inc=1, device_id=(z + 1, me), device_id_type=MESH)

    line = (z + spread - 1) // spread + (2 * spread - 2 - z) // spread
    pl.semaphore_wait(barrier, 3 + line)

    chunks = 2
    chunk_rows = tokens // chunks

    def along(item, owner, step, own):
        if item < chunks:
            rows = pl.ds(item * chunk_rows, chunk_rows)
            target = pair_buf.at[owner, rows]
            source = pair_hbm.at[0, rows] if own else target
        else:
            target = rope_buf.at[owner]
            source = rope_hbm.at[0] if own else target
        return pltpu.make_async_remote_copy(
            src_ref=source,
            dst_ref=target,
            send_sem=zsend_sem.at[0 if step < 0 else 1, owner, item],
            recv_sem=zrecv_sem.at[owner, item],
            device_id=(z + step, me),
            device_id_type=MESH,
        )

    def send_along(owner, own, step, item):
        @pl.when((z > 0) if step < 0 else (z < spread - 1))
        def _():
            along(item, owner, step, own).start()

    items = range(chunks + 1)
    for item in items:
        for step in (-1, 1):
            send_along(z, True, step, item)

    def relay_along(distance, item):
        for side in (1, -1):
            owner = z + side * distance

            @pl.when((owner >= 0) & (owner < spread))
            def _():
                along(item, owner, -side, False).wait_recv()
                send_along(owner, False, -side, item)

    def across(index, kind):
        a, start, width = pieces[index]
        cols = pl.ds(start, width)
        target_of = {
            0: (me, None, peer_p),
            1: (me, None, peer_x),
            2: (me, None, peer_y),
            3: (peer_x, None, peer_p),
            4: (peer_y, None, peer_p),
            5: (peer_x, 0, peer_y),
            6: (peer_y, 1, peer_x),
            7: (diagonal, 0, peer_p),
            8: (diagonal, 1, peer_p),
        }
        owner, half, device = target_of[kind]
        target = gathered[a].at[rows_of(a, owner, half), cols]
        source = weights[a].at[:, cols] if kind < 3 else target
        return pltpu.make_async_remote_copy(
            src_ref=source,
            dst_ref=target,
            send_sem=send_sem.at[index, kind],
            recv_sem=recv_sem.at[index, kind],
            device_id=(z, device),
            device_id_type=MESH,
        )

    def arrived(index, kind):
        a, start, width = pieces[index]
        owner, half = {
            0: (peer_p, None),
            1: (peer_x, None),
            2: (peer_y, None),
            3: (peer_x + flip_p, None),
            4: (peer_y + flip_p, None),
            5: (diagonal, 0),
            6: (diagonal, 1),
            7: (diagonal + flip_p, 0),
            8: (diagonal + flip_p, 1),
        }[kind]
        target = gathered[a].at[rows_of(a, owner, half), pl.ds(start, width)]
        pltpu.make_async_remote_copy(
            src_ref=target,
            dst_ref=target,
            send_sem=send_sem.at[index, kind],
            recv_sem=recv_sem.at[index, kind],
            device_id=(z, peer_p),
            device_id_type=MESH,
        ).wait_recv()

    def send_own(index):
        for kind in (1, 2, 0):
            across(index, kind).start()

    def relay(index):
        arrived(index, 1)
        across(index, 5).start()
        across(index, 3).start()
        arrived(index, 2)
        across(index, 6).start()
        across(index, 4).start()

    def hand_over(index):
        for half in (0, 1):
            arrived(index, 5 + half)
            across(index, 7 + half).start()

    def complete(index):
        for kind in (0, 3, 4, 7, 8):
            arrived(index, kind)

    for index in range(4):
        send_own(index)

    def normed(values, gain):
        values = values.astype(jnp.float32)
        scaled = values * lax.rsqrt(jnp.mean(values * values, axis=-1, keepdims=True) + EPSILON)
        return (scaled * gain).astype(jnp.bfloat16)

    for copy in local:
        copy.wait()
    for copy in own_weights:
        copy.wait()
    query_normed = normed(query_buf[...], qgain[...])
    own_table = ktab[pl.ds(pl.multiple_of(z * tokens, tokens), tokens)]
    for table, plain in ((ntab, PLAIN_NARROW), (btab, PLAIN_BROAD)):
        for index, values in enumerate(wide_tables(own_table, plain, heads)):
            table[index] = values

    relay(0)
    send_own(4)
    relay(1)
    for item in items:
        relay_along(1, item)
    relay(2)
    relay(3)
    send_own(5)
    send_own(6)
    hand_over(0)
    hand_over(1)
    for item in items:
        relay_along(2, item)
    relay(4)
    hand_over(2)
    for distance in range(3, spread):
        for item in items:
            relay_along(distance, item)
    hand_over(3)
    relay(5)
    for index in range(3):
        complete(index)

    for block in range(spread):
        rows = pl.ds(block * tokens, tokens)
        pair_normed[rows] = normed(pair_buf[block], pgain[...])
        plain = rope_buf[block].astype(jnp.float32).T
        halfway = ROTARY // 2
        swapped = jnp.concatenate([plain[:, halfway:], plain[:, :halfway]], axis=1)
        rope_keys[rows] = (
            plain * ktab[rows, :ROTARY] + swapped * ktab[rows, ROTARY:]
        ).astype(jnp.bfloat16)

    def product(left, right):
        return jnp.dot(left, right, preferred_element_type=jnp.float32)

    def project(sums, array, start, width):
        cols = pl.ds(start, width)
        sums[:, cols] = product(query_normed, gathered[array][:, cols])

    def rotated(sums, table, start, stop):
        halfway, cols = ROTARY // 2, pl.ds(start, stop - start)
        values = sums[:, cols]
        return (
            values * table[0, :, cols]
            + pltpu.roll(values, stop - start - halfway, 1) * table[1, :, cols]
            + pltpu.roll(values, halfway, 1) * table[2, :, cols]
        ).astype(jnp.bfloat16)

    def attend(queries, start, keys, values, plain, which):
        width = plain + ROTARY
        factor = width ** (-0.5) * math.log2(math.e)
        attended = []
        for head in which:
            query = queries[:, head * width - start : (head + 1) * width - start]
            key = jnp.concatenate(
                [keys[:, head * plain : (head + 1) * plain], rope_keys[...]], axis=1
            )
            scores = lax.dot_general(
                query, key, (((1,), (1,)), ((), ())), preferred_element_type=jnp.float32
            )
            shifted = jnp.exp2((scores - jnp.max(scores, axis=-1, keepdims=True)) * factor)
            totals = jnp.sum(shifted, axis=-1, keepdims=True)
            mixed = product(
                shifted.astype(jnp.bfloat16), values[:, head * VALUE_SIZE : (head + 1) * VALUE_SIZE]
            )
            attended.append((mixed / totals).astype(jnp.bfloat16).astype(jnp.float32))
        return attended

    def finish_group(attended, out):
        flat = jnp.concatenate(attended, axis=1)
        scaled = flat * lax.rsqrt(jnp.mean(flat * flat, axis=-1, keepdims=True) + EPSILON)
        out[0] = scaled.astype(jnp.bfloat16)

    project(narrow_sums, NQ, 0, columns_all[NQ])
    narrow_queries = rotated(narrow_sums, ntab, 0, columns_all[NQ])
    narrow_keys = product(pair_normed[...], gathered[NK][...]).astype(jnp.bfloat16)
    narrow_values = product(pair_normed[...], gathered[NV][...]).astype(jnp.bfloat16)
    relay(6)
    hand_over(4)
    complete(3)
    broad_keys = product(pair_normed[...], gathered[BK][...]).astype(jnp.bfloat16)
    hand_over(5)
    finish_group(
        attend(narrow_queries, 0, narrow_keys, narrow_values, PLAIN_NARROW, range(heads)),
        narrow_out,
    )
    hand_over(6)
    complete(4)
    broad_values = product(pair_normed[...], gathered[BV][...]).astype(jnp.bfloat16)
    complete(5)
    width_broad = PLAIN_BROAD + ROTARY
    early = split // width_broad
    project(broad_sums, BQ, 0, split)
    attended = attend(
        rotated(broad_sums, btab, 0, split), 0, broad_keys, broad_values, PLAIN_BROAD, range(early)
    )
    complete(6)
    project(broad_sums, BQ, split, columns_all[BQ] - split)
    start = early * width_broad // LANES * LANES
    attended += attend(
        rotated(broad_sums, btab, start, columns_all[BQ]),
        start,
        broad_keys,
        broad_values,
        PLAIN_BROAD,
        range(early, heads),
    )
    finish_group(attended, broad_out)

    for index in range(len(pieces)):
        for kind in range(KINDS):
            across(index, kind).wait_send()
    for item in items:
        for step in (-1, 1):
            for distance in range(spread):
                owner = z - step * distance

                @pl.when(
                    (owner >= 0)
                    & (owner < spread)
                    & ((z > 0) if step < 0 else (z < spread - 1))
                )
                def _():
                    along(item, owner, step, False).wait_send()


def hand_out(narrow, broad, narrow_out, broad_out, sems):
    copies = [
        pltpu.make_async_copy(narrow, narrow_out, sems.at[0]),
        pltpu.make_async_copy(broad, broad_out, sems.at[1]),
    ]
    for copy in copies:
        copy.start()
    for copy in copies:
        copy.wait()


def fused_call(
    spread,
    query_latent,
    keyvalue_latent,
    rope_key,
    query_gain,
    keyvalue_gain,
    narrow_query,
    broad_query,
    narrow_key,
    narrow_value,
    broad_key,
    broad_value,
):
    tokens, query_rank = query_latent.shape[1:]
    pair_rank = keyvalue_latent.shape[2]
    length = tokens * spread
    heads = narrow_value.shape[1] // VALUE_SIZE
    weights = (narrow_key, narrow_value, narrow_query, broad_key, broad_value, broad_query)
    peers = lax.axis_size("dp")
    ktab = key_table(length)
    operands = (
        query_latent,
        keyvalue_latent,
        jnp.swapaxes(rope_key, 1, 2),
        query_gain,
        keyvalue_gain,
        *weights,
        jnp.asarray(ktab),
    )
    out = jax.ShapeDtypeStruct((1, tokens, heads * VALUE_SIZE), jnp.bfloat16)
    bf16, f32 = jnp.bfloat16, jnp.float32
    mixed = pl.pallas_call(
        functools.partial(fused, spread, heads),
        out_shape=(out, out),
        in_specs=[pl.BlockSpec(memory_space=pltpu.HBM)] * len(operands),
        out_specs=[pl.BlockSpec(memory_space=pltpu.VMEM)] * 2,
        scratch_shapes=[
            *[pltpu.VMEM((w.shape[0] * peers, w.shape[1]), bf16) for w in weights],
            pltpu.VMEM((tokens, query_rank), bf16),
            pltpu.VMEM((spread, tokens, pair_rank), bf16),
            pltpu.VMEM((spread, ROTARY, tokens), bf16),
            pltpu.VMEM((1, query_rank), f32),
            pltpu.VMEM((1, pair_rank), f32),
            pltpu.VMEM((3, tokens, narrow_query.shape[1]), f32),
            pltpu.VMEM((3, tokens, broad_query.shape[1]), f32),
            pltpu.VMEM(ktab.shape, f32),
            pltpu.VMEM((length, pair_rank), bf16),
            pltpu.VMEM((length, ROTARY), bf16),
            pltpu.VMEM((tokens, narrow_query.shape[1]), f32),
            pltpu.VMEM((tokens, broad_query.shape[1]), f32),
            pltpu.SemaphoreType.DMA((7, KINDS)),
            pltpu.SemaphoreType.DMA((7, KINDS)),
            pltpu.SemaphoreType.DMA((2, spread, 3)),
            pltpu.SemaphoreType.DMA((spread, 3)),
            pltpu.SemaphoreType.DMA((6,)),
            pltpu.SemaphoreType.DMA((6,)),
        ],
        compiler_params=pltpu.CompilerParams(
            collective_id=0, has_side_effects=True, vmem_limit_bytes=48 * 2**20
        ),
    )(*[pltpu.with_memory_space_constraint(operand, pltpu.HBM) for operand in operands])
    return pl.pallas_call(
        hand_out,
        out_shape=(out, out),
        in_specs=[pl.BlockSpec(memory_space=pltpu.VMEM)] * 2,
        out_specs=[pl.BlockSpec(memory_space=pltpu.HBM)] * 2,
        scratch_shapes=[pltpu.SemaphoreType.DMA((2,))],
        compiler_params=pltpu.CompilerParams(vmem_limit_bytes=2**20),
    )(*mixed)


def solution(mesh):
    in_specs = (
        P("dp", "sp", None),
        P("dp", "sp", None),
        P("dp", "sp", None),
        P(),
        P(),
        P("dp", None),
        P("dp", None),
        P("dp", None),
        P("dp", None),
        P("dp", None),
        P("dp", None),
    )
    out_specs = (P("dp", "sp", None), P("dp", "sp", None))
    spread = mesh.shape["sp"]

    def choose(*arrays):
        rows = [a.shape[0] for a in arrays[5:]]
        fits = lax.axis_size("dp") == 2**3 and all(r % (2 * ROW_TILE) == 0 for r in rows)
        if fits:
            return fused_call(spread, *arrays)
        return on_device(*arrays)

    return jax.shard_map(
        choose, mesh=mesh, in_specs=in_specs, out_specs=out_specs, check_vma=False
    )
```

```python
import functools
import math

import jax
import jax.numpy as jnp
import numpy as np
from jax import lax
from jax.experimental import pallas as pl
from jax.experimental.pallas import tpu as pltpu
from jax.sharding import PartitionSpec as P

PLAIN_NARROW = 64
PLAIN_BROAD = 128
ROTARY = 32
VALUE_SIZE = 64


EPSILON = 1e-06
ROTARY_BASE = 10000.0


def normalize(latent, gain_row):
    values = latent.astype(jnp.float32)
    scaled = values * lax.rsqrt(jnp.mean(values * values, axis=-1, keepdims=True) + EPSILON)
    return (scaled * gain_row).astype(jnp.bfloat16)


def rotate(values, positions):
    halfway = ROTARY // 2
    frequency = ROTARY_BASE ** (-jnp.arange(halfway, dtype=jnp.float32) / halfway)
    angles = positions[:, None] * frequency[None, :]
    cosine = jnp.cos(angles)[:, None, :]
    sine_part = jnp.sin(angles)[:, None, :]
    width = values.shape[-1]
    plain_part = values[..., : width - ROTARY]
    first_half = values[..., width - ROTARY : width - halfway]
    second_half = values[..., width - halfway :]
    return jnp.concatenate(
        [
            plain_part,
            first_half * cosine - second_half * sine_part,
            first_half * sine_part + second_half * cosine,
        ],
        axis=-1,
    )


def make_fold(latent, pieces):
    return tuple(
        (jnp.dot(latent, weight_rows, preferred_element_type=jnp.float32) for weight_rows in pieces)
    )


def arrange(sums, width, positions, groups, with_rotary):
    row_count = positions.shape[0]
    shaped = sums.reshape(row_count, -1, width)
    if with_rotary:
        shaped = rotate(shaped, positions)
    shaped = shaped.astype(jnp.bfloat16)
    return shaped.reshape(row_count, groups, shaped.shape[1] // groups, width)


def attend_group(queries, keys_plain, values, rope_keys, factor):
    length = queries.shape[0]
    block_rows = 512
    key_whole = jnp.concatenate([keys_plain[:, 0, :], rope_keys], axis=1)
    value_head = values[:, 0, :]

    def one_block(query_block):
        scores = (
            jnp.einsum("qd,kd->qk", query_block, key_whole, preferred_element_type=jnp.float32)
            * factor
        )
        shifted = jnp.exp(scores - jnp.max(scores, axis=-1, keepdims=True))
        totals = jnp.sum(shifted, axis=-1, keepdims=True)
        mixed = jnp.dot(
            shifted.astype(jnp.bfloat16), value_head, preferred_element_type=jnp.float32
        )
        return (mixed / totals).astype(jnp.bfloat16)

    blocks = lax.map(one_block, queries[:, 0, :].reshape(length // block_rows, block_rows, -1))
    results = [blocks.reshape(length, -1)]
    return jnp.stack(results, axis=1)


def attend_both(members, rope_keys):
    query_first, key_first, value_first, query_second, key_second, value_second = members
    mixed_first = attend_group(
        query_first[:, 0],
        key_first[:, 0],
        value_first[:, 0],
        rope_keys,
        (PLAIN_NARROW + ROTARY) ** (-0.5),
    )
    mixed_second = attend_group(
        query_second[:, 0],
        key_second[:, 0],
        value_second[:, 0],
        rope_keys,
        (PLAIN_BROAD + ROTARY) ** (-0.5),
    )
    return (mixed_first[:, None], mixed_second[:, None])


def finish(mixed):
    flattened = mixed.reshape(mixed.shape[0], -1).astype(jnp.float32)
    scaled = flattened * lax.rsqrt(
        jnp.mean(flattened * flattened, axis=-1, keepdims=True) + EPSILON
    )
    return scaled.astype(jnp.bfloat16)[None]


def on_device(
    query_latent,
    keyvalue_latent,
    rope_key,
    query_gain,
    keyvalue_gain,
    narrow_query,
    broad_query,
    narrow_key,
    narrow_value,
    broad_key,
    broad_value,
):
    tokens = query_latent.shape[1]
    spread = lax.axis_size("sp")
    device_index = lax.axis_index("sp")
    width_narrow = PLAIN_NARROW + ROTARY
    width_broad = PLAIN_BROAD + ROTARY
    query_normed = normalize(query_latent[0], query_gain)
    pair_normed = normalize(keyvalue_latent[0], keyvalue_gain)
    own_positions = (device_index * tokens + jnp.arange(tokens, dtype=jnp.int32)).astype(
        jnp.float32
    )
    rope_own = rotate(rope_key[0].astype(jnp.float32)[:, None, :], own_positions)[:, 0, :].astype(
        jnp.bfloat16
    )
    query_all, pair_all, rope_all = (
        lax.all_gather(query_normed, "sp", axis=0, tiled=True),
        lax.all_gather(pair_normed, "sp", axis=0, tiled=True),
        lax.all_gather(rope_own, "sp", axis=0, tiled=True),
    )
    length = tokens * spread
    all_positions = jnp.arange(length, dtype=jnp.int32).astype(jnp.float32)

    def own_columns(weight, width):
        count = weight.shape[1] // (width * spread)
        return lax.dynamic_slice_in_dim(weight, device_index * count * width, count * width, 1)

    own_narrow_query = own_columns(narrow_query, width_narrow)
    own_broad_query = own_columns(broad_query, width_broad)
    own_narrow_key = own_columns(narrow_key, PLAIN_NARROW)
    own_narrow_value = own_columns(narrow_value, VALUE_SIZE)
    own_broad_key = own_columns(broad_key, PLAIN_BROAD)
    own_broad_value = own_columns(broad_value, VALUE_SIZE)
    query_sums = make_fold(
        query_all,
        (
            lax.all_gather(own_narrow_query, "dp", axis=0, tiled=True),
            lax.all_gather(own_broad_query, "dp", axis=0, tiled=True),
        ),
    )
    pair_sums = make_fold(
        pair_all,
        (
            lax.all_gather(own_narrow_key, "dp", axis=0, tiled=True),
            lax.all_gather(own_narrow_value, "dp", axis=0, tiled=True),
            lax.all_gather(own_broad_key, "dp", axis=0, tiled=True),
            lax.all_gather(own_broad_value, "dp", axis=0, tiled=True),
        ),
    )
    members = (
        arrange(query_sums[0], width_narrow, all_positions, 1, True),
        arrange(pair_sums[0], PLAIN_NARROW, all_positions, 1, False),
        arrange(pair_sums[1], VALUE_SIZE, all_positions, 1, False),
        arrange(query_sums[1], width_broad, all_positions, 1, True),
        arrange(pair_sums[2], PLAIN_BROAD, all_positions, 1, False),
        arrange(pair_sums[3], VALUE_SIZE, all_positions, 1, False),
    )
    mixed_first, mixed_second = attend_both(members, rope_all)
    back_first, back_second = (
        lax.all_to_all(mixed_first, "sp", split_axis=0, concat_axis=1, tiled=True),
        lax.all_to_all(mixed_second, "sp", split_axis=0, concat_axis=1, tiled=True),
    )
    return (finish(back_first), finish(back_second))


MESH = pl.DeviceIdType.MESH
ROW_TILE = 16
LANES = 128
NK, NV, NQ, BK, BV, BQ = range(6)
KINDS = 9


def rotary_tables(length):
    halfway = ROTARY // 2
    frequency = (
        np.float32(ROTARY_BASE) ** (-np.arange(halfway, dtype=np.float32) / np.float32(halfway))
    ).astype(np.float32)
    angles = np.arange(length, dtype=np.float32)[:, None] * frequency[None, :]
    cosine = np.cos(angles.astype(np.float64)).astype(np.float32)
    sine = np.sin(angles.astype(np.float64)).astype(np.float32)
    return cosine, sine


def key_table(length):
    cosine, sine = rotary_tables(length)
    return np.concatenate([cosine, cosine, -sine, sine], 1)


def wide_tables(table, plain, heads):
    rows, halfway = table.shape[0], ROTARY // 2
    ones = jnp.ones((rows, plain), jnp.float32)
    zeros = jnp.zeros((rows, plain), jnp.float32)
    zero = jnp.zeros((rows, halfway), jnp.float32)
    keep = [ones, table[:, :ROTARY]]
    ahead = [zeros, table[:, ROTARY : ROTARY + halfway], zero]
    behind = [zeros, zero, table[:, ROTARY + halfway :]]
    return [jnp.concatenate(parts * heads, axis=1) for parts in (keep, ahead, behind)]


def fused(
    spread,
    heads,
    query_hbm,
    pair_hbm,
    rope_hbm,
    qgain_hbm,
    pgain_hbm,
    w0,
    w1,
    w2,
    w3,
    w4,
    w5,
    ktab_hbm,
    narrow_out,
    broad_out,
    g0,
    g1,
    g2,
    g3,
    g4,
    g5,
    query_buf,
    pair_buf,
    rope_buf,
    qgain,
    pgain,
    ntab,
    btab,
    ktab,
    pair_normed,
    rope_keys,
    narrow_sums,
    broad_sums,
    send_sem,
    recv_sem,
    zsend_sem,
    zrecv_sem,
    local_sem,
    wlocal_sem,
):
    weights = (w0, w1, w2, w3, w4, w5)
    gathered = (g0, g1, g2, g3, g4, g5)
    tokens = query_hbm.shape[1]
    z = lax.axis_index("sp")
    me = lax.axis_index("dp")
    core = me % 2
    flip_p = 1 - 2 * core
    flip_x = 2 * (1 - 2 * ((me // 2) % 2))
    flip_y = 4 * (1 - 2 * (me // 4))
    peer_p, peer_x, peer_y = me + flip_p, me + flip_x, me + flip_y
    diagonal = me + flip_x + flip_y

    columns_all = [w.shape[1] for w in weights]
    pieces = [(a, 0, columns_all[a]) for a in (NK, NV, NQ, BK, BV)]
    split = -(-(columns_all[BQ] // 2) // LANES) * LANES
    pieces += [(BQ, 0, split), (BQ, split, columns_all[BQ] - split)]

    local = [
        pltpu.make_async_copy(pair_hbm.at[0], pair_buf.at[z], local_sem.at[0]),
        pltpu.make_async_copy(rope_hbm.at[0], rope_buf.at[z], local_sem.at[1]),
        pltpu.make_async_copy(query_hbm.at[0], query_buf, local_sem.at[2]),
        pltpu.make_async_copy(qgain_hbm, qgain.at[0], local_sem.at[3]),
        pltpu.make_async_copy(pgain_hbm, pgain.at[0], local_sem.at[4]),
        pltpu.make_async_copy(ktab_hbm, ktab, local_sem.at[5]),
    ]

    def rows_of(array, owner, half=None):
        rows = weights[array].shape[0]
        if half is None:
            return pl.ds(pl.multiple_of(owner * rows, rows), rows)
        part = rows // 2
        return pl.ds(pl.multiple_of(owner * rows + half * part, part), part)

    own_weights = [
        pltpu.make_async_copy(
            weights[a], gathered[a].at[rows_of(a, me)], wlocal_sem.at[a]
        )
        for a in range(len(weights))
    ]
    for copy in local + own_weights:
        copy.start()

    barrier = pltpu.get_barrier_semaphore()
    for peer in (peer_p, peer_x, peer_y):
        pl.semaphore_signal(barrier, inc=1, device_id=(z, peer), device_id_type=MESH)

    @pl.when(z > 0)
    def _():
        pl.semaphore_signal(barrier, inc=1, device_id=(z - 1, me), device_id_type=MESH)

    @pl.when(z < spread - 1)
    def _():
        pl.semaphore_signal(barrier, inc=1, device_id=(z + 1, me), device_id_type=MESH)

    line = (z + spread - 1) // spread + (2 * spread - 2 - z) // spread
    pl.semaphore_wait(barrier, 3 + line)

    chunks = 2
    chunk_rows = tokens // chunks

    def along(item, owner, step, own):
        if item < chunks:
            rows = pl.ds(item * chunk_rows, chunk_rows)
            target = pair_buf.at[owner, rows]
            source = pair_hbm.at[0, rows] if own else target
        else:
            target = rope_buf.at[owner]
            source = rope_hbm.at[0] if own else target
        return pltpu.make_async_remote_copy(
            src_ref=source,
            dst_ref=target,
            send_sem=zsend_sem.at[0 if step < 0 else 1, owner, item],
            recv_sem=zrecv_sem.at[owner, item],
            device_id=(z + step, me),
            device_id_type=MESH,
        )

    def send_along(owner, own, step, item):
        @pl.when((z > 0) if step < 0 else (z < spread - 1))
        def _():
            along(item, owner, step, own).start()

    items = range(chunks + 1)
    for item in items:
        for step in (-1, 1):
            send_along(z, True, step, item)

    def relay_along(distance, item):
        for side in (1, -1):
            owner = z + side * distance

            @pl.when((owner >= 0) & (owner < spread))
            def _():
                along(item, owner, -side, False).wait_recv()
                send_along(owner, False, -side, item)

    def across(index, kind):
        a, start, width = pieces[index]
        cols = pl.ds(start, width)
        target_of = {
            0: (me, None, peer_p),
            1: (me, None, peer_x),
            2: (me, None, peer_y),
            3: (peer_x, None, peer_p),
            4: (peer_y, None, peer_p),
            5: (peer_x, 0, peer_y),
            6: (peer_y, 1, peer_x),
            7: (diagonal, 0, peer_p),
            8: (diagonal, 1, peer_p),
        }
        owner, half, device = target_of[kind]
        target = gathered[a].at[rows_of(a, owner, half), cols]
        source = weights[a].at[:, cols] if kind < 3 else target
        return pltpu.make_async_remote_copy(
            src_ref=source,
            dst_ref=target,
            send_sem=send_sem.at[index, kind],
            recv_sem=recv_sem.at[index, kind],
            device_id=(z, device),
            device_id_type=MESH,
        )

    def arrived(index, kind):
        a, start, width = pieces[index]
        owner, half = {
            0: (peer_p, None),
            1: (peer_x, None),
            2: (peer_y, None),
            3: (peer_x + flip_p, None),
            4: (peer_y + flip_p, None),
            5: (diagonal, 0),
            6: (diagonal, 1),
            7: (diagonal + flip_p, 0),
            8: (diagonal + flip_p, 1),
        }[kind]
        target = gathered[a].at[rows_of(a, owner, half), pl.ds(start, width)]
        pltpu.make_async_remote_copy(
            src_ref=target,
            dst_ref=target,
            send_sem=send_sem.at[index, kind],
            recv_sem=recv_sem.at[index, kind],
            device_id=(z, peer_p),
            device_id_type=MESH,
        ).wait_recv()

    def send_own(index):
        for kind in (1, 2, 0):
            across(index, kind).start()

    def relay(index):
        arrived(index, 1)
        across(index, 5).start()
        across(index, 3).start()
        arrived(index, 2)
        across(index, 6).start()
        across(index, 4).start()

    def hand_over(index):
        for half in (0, 1):
            arrived(index, 5 + half)
            across(index, 7 + half).start()

    def complete(index):
        for kind in (0, 3, 4, 7, 8):
            arrived(index, kind)

    for index in range(3):
        send_own(index)

    def normed(values, gain):
        values = values.astype(jnp.float32)
        scaled = values * lax.rsqrt(jnp.mean(values * values, axis=-1, keepdims=True) + EPSILON)
        return (scaled * gain).astype(jnp.bfloat16)

    for copy in local:
        copy.wait()
    for copy in own_weights:
        copy.wait()
    query_normed = normed(query_buf[...], qgain[...])
    own_table = ktab[pl.ds(pl.multiple_of(z * tokens, tokens), tokens)]
    for table, plain in ((ntab, PLAIN_NARROW), (btab, PLAIN_BROAD)):
        for index, values in enumerate(wide_tables(own_table, plain, heads)):
            table[index] = values

    relay(0)
    send_own(3)
    relay(1)
    send_own(4)
    for item in items:
        relay_along(1, item)
    relay(2)
    send_own(5)
    relay(3)
    send_own(6)
    hand_over(0)
    hand_over(1)
    for item in items:
        relay_along(2, item)
    relay(4)
    hand_over(2)
    for distance in range(3, spread):
        for item in items:
            relay_along(distance, item)
    hand_over(3)
    relay(5)
    for index in range(3):
        complete(index)

    for block in range(spread):
        rows = pl.ds(block * tokens, tokens)
        pair_normed[rows] = normed(pair_buf[block], pgain[...])
        plain = rope_buf[block].astype(jnp.float32).T
        halfway = ROTARY // 2
        swapped = jnp.concatenate([plain[:, halfway:], plain[:, :halfway]], axis=1)
        rope_keys[rows] = (
            plain * ktab[rows, :ROTARY] + swapped * ktab[rows, ROTARY:]
        ).astype(jnp.bfloat16)

    def product(left, right):
        return jnp.dot(left, right, preferred_element_type=jnp.float32)

    def project(sums, array, start, width):
        cols = pl.ds(start, width)
        sums[:, cols] = product(query_normed, gathered[array][:, cols])

    def rotated(sums, table, start, stop):
        halfway, cols = ROTARY // 2, pl.ds(start, stop - start)
        values = sums[:, cols]
        return (
            values * table[0, :, cols]
            + pltpu.roll(values, stop - start - halfway, 1) * table[1, :, cols]
            + pltpu.roll(values, halfway, 1) * table[2, :, cols]
        ).astype(jnp.bfloat16)

    def attend(queries, start, keys, values, plain, which):
        width = plain + ROTARY
        factor = width ** (-0.5) * math.log2(math.e)
        attended = []
        for head in which:
            query = queries[:, head * width - start : (head + 1) * width - start]
            key = jnp.concatenate(
                [keys[:, head * plain : (head + 1) * plain], rope_keys[...]], axis=1
            )
            scores = lax.dot_general(
                query, key, (((1,), (1,)), ((), ())), preferred_element_type=jnp.float32
            )
            shifted = jnp.exp2((scores - jnp.max(scores, axis=-1, keepdims=True)) * factor)
            totals = jnp.sum(shifted, axis=-1, keepdims=True)
            mixed = product(
                shifted.astype(jnp.bfloat16), values[:, head * VALUE_SIZE : (head + 1) * VALUE_SIZE]
            )
            attended.append((mixed / totals).astype(jnp.bfloat16).astype(jnp.float32))
        return attended

    def finish_group(attended, out):
        flat = jnp.concatenate(attended, axis=1)
        scaled = flat * lax.rsqrt(jnp.mean(flat * flat, axis=-1, keepdims=True) + EPSILON)
        out[0] = scaled.astype(jnp.bfloat16)

    project(narrow_sums, NQ, 0, columns_all[NQ])
    narrow_queries = rotated(narrow_sums, ntab, 0, columns_all[NQ])
    narrow_keys = product(pair_normed[...], gathered[NK][...]).astype(jnp.bfloat16)
    narrow_values = product(pair_normed[...], gathered[NV][...]).astype(jnp.bfloat16)
    relay(6)
    hand_over(4)
    complete(3)
    broad_keys = product(pair_normed[...], gathered[BK][...]).astype(jnp.bfloat16)
    hand_over(5)
    finish_group(
        attend(narrow_queries, 0, narrow_keys, narrow_values, PLAIN_NARROW, range(heads)),
        narrow_out,
    )
    hand_over(6)
    complete(4)
    broad_values = product(pair_normed[...], gathered[BV][...]).astype(jnp.bfloat16)
    complete(5)
    width_broad = PLAIN_BROAD + ROTARY
    early = split // width_broad
    project(broad_sums, BQ, 0, split)
    attended = attend(
        rotated(broad_sums, btab, 0, split), 0, broad_keys, broad_values, PLAIN_BROAD, range(early)
    )
    complete(6)
    project(broad_sums, BQ, split, columns_all[BQ] - split)
    start = early * width_broad // LANES * LANES
    attended += attend(
        rotated(broad_sums, btab, start, columns_all[BQ]),
        start,
        broad_keys,
        broad_values,
        PLAIN_BROAD,
        range(early, heads),
    )
    finish_group(attended, broad_out)

    for index in range(len(pieces)):
        for kind in range(KINDS):
            across(index, kind).wait_send()
    for item in items:
        for step in (-1, 1):
            for distance in range(spread):
                owner = z - step * distance

                @pl.when(
                    (owner >= 0)
                    & (owner < spread)
                    & ((z > 0) if step < 0 else (z < spread - 1))
                )
                def _():
                    along(item, owner, step, False).wait_send()


def hand_out(narrow, broad, narrow_out, broad_out, sems):
    copies = [
        pltpu.make_async_copy(narrow, narrow_out, sems.at[0]),
        pltpu.make_async_copy(broad, broad_out, sems.at[1]),
    ]
    for copy in copies:
        copy.start()
    for copy in copies:
        copy.wait()


def fused_call(
    spread,
    query_latent,
    keyvalue_latent,
    rope_key,
    query_gain,
    keyvalue_gain,
    narrow_query,
    broad_query,
    narrow_key,
    narrow_value,
    broad_key,
    broad_value,
):
    tokens, query_rank = query_latent.shape[1:]
    pair_rank = keyvalue_latent.shape[2]
    length = tokens * spread
    heads = narrow_value.shape[1] // VALUE_SIZE
    weights = (narrow_key, narrow_value, narrow_query, broad_key, broad_value, broad_query)
    peers = lax.axis_size("dp")
    ktab = key_table(length)
    operands = (
        query_latent,
        keyvalue_latent,
        jnp.swapaxes(rope_key, 1, 2),
        query_gain,
        keyvalue_gain,
        *weights,
        jnp.asarray(ktab),
    )
    out = jax.ShapeDtypeStruct((1, tokens, heads * VALUE_SIZE), jnp.bfloat16)
    bf16, f32 = jnp.bfloat16, jnp.float32
    mixed = pl.pallas_call(
        functools.partial(fused, spread, heads),
        out_shape=(out, out),
        in_specs=[pl.BlockSpec(memory_space=pltpu.HBM)] * len(operands),
        out_specs=[pl.BlockSpec(memory_space=pltpu.VMEM)] * 2,
        scratch_shapes=[
            *[pltpu.VMEM((w.shape[0] * peers, w.shape[1]), bf16) for w in weights],
            pltpu.VMEM((tokens, query_rank), bf16),
            pltpu.VMEM((spread, tokens, pair_rank), bf16),
            pltpu.VMEM((spread, ROTARY, tokens), bf16),
            pltpu.VMEM((1, query_rank), f32),
            pltpu.VMEM((1, pair_rank), f32),
            pltpu.VMEM((3, tokens, narrow_query.shape[1]), f32),
            pltpu.VMEM((3, tokens, broad_query.shape[1]), f32),
            pltpu.VMEM(ktab.shape, f32),
            pltpu.VMEM((length, pair_rank), bf16),
            pltpu.VMEM((length, ROTARY), bf16),
            pltpu.VMEM((tokens, narrow_query.shape[1]), f32),
            pltpu.VMEM((tokens, broad_query.shape[1]), f32),
            pltpu.SemaphoreType.DMA((7, KINDS)),
            pltpu.SemaphoreType.DMA((7, KINDS)),
            pltpu.SemaphoreType.DMA((2, spread, 3)),
            pltpu.SemaphoreType.DMA((spread, 3)),
            pltpu.SemaphoreType.DMA((6,)),
            pltpu.SemaphoreType.DMA((6,)),
        ],
        compiler_params=pltpu.CompilerParams(
            collective_id=0, has_side_effects=True, vmem_limit_bytes=48 * 2**20
        ),
    )(*[pltpu.with_memory_space_constraint(operand, pltpu.HBM) for operand in operands])
    return pl.pallas_call(
        hand_out,
        out_shape=(out, out),
        in_specs=[pl.BlockSpec(memory_space=pltpu.VMEM)] * 2,
        out_specs=[pl.BlockSpec(memory_space=pltpu.HBM)] * 2,
        scratch_shapes=[pltpu.SemaphoreType.DMA((2,))],
        compiler_params=pltpu.CompilerParams(vmem_limit_bytes=2**20),
    )(*mixed)


def solution(mesh):
    in_specs = (
        P("dp", "sp", None),
        P("dp", "sp", None),
        P("dp", "sp", None),
        P(),
        P(),
        P("dp", None),
        P("dp", None),
        P("dp", None),
        P("dp", None),
        P("dp", None),
        P("dp", None),
    )
    out_specs = (P("dp", "sp", None), P("dp", "sp", None))
    spread = mesh.shape["sp"]

    def choose(*arrays):
        rows = [a.shape[0] for a in arrays[5:]]
        fits = lax.axis_size("dp") == 2**3 and all(r % (2 * ROW_TILE) == 0 for r in rows)
        if fits:
            return fused_call(spread, *arrays)
        return on_device(*arrays)

    return jax.shard_map(
        choose, mesh=mesh, in_specs=in_specs, out_specs=out_specs, check_vma=False
    )
```
